32 devices in a mesh: sp: 4 (over y, x), dp: 8 (over z, core).
Axes of the slice: x: 2, y: 2, z: 4, core: 2. Of those that a mesh axis runs over, the one named last changes fastest.
Arguments:
- tokens: bfloat16 [8, 1024, 2048], P('dp', 'sp'), may hold values from -200 to 200
- w_qdown: bfloat16 [2048, 512], P('dp'), may hold values from -0.125 to 0.125
- w_kvdown: bfloat16 [2048, 512], P('dp'), may hold values from -0.125 to 0.125
- w_rotary: bfloat16 [2048, 64], replicated, may hold values from -0.125 to 0.125
- q_gain: float32 [512], replicated, may hold values from 0.1 to 1.9
- kv_gain: float32 [512], replicated, may hold values from 0.1 to 1.9
- w_qup: bfloat16 [512, 3072], P('dp'), may hold values from -1 to 1
- w_kvup: bfloat16 [512, 4096], P('dp'), may hold values from -1 to 1
- w_out: bfloat16 [2048, 2048], P(None, 'dp'), may hold values from -0.125 to 0.125
- out_gain: float32 [2048], replicated, may hold values from 0.1 to 1.9
Outputs:
- mixed: bfloat16 [8, 1024, 2048], P('dp', 'sp')
The draws below stay inside these ranges and needn't reach their ends.
All inputs are finite; a program needn't handle non-finite values.
Results may differ from the reference program's by a relative error of at most 0.01.
The reference program's roundings to bfloat16 on the way count: a program that leaves them out, or rounds other values in their place, can miss the bound.
Values may be sent and summed in bfloat16 or wider, within the bound.
A program may use at most 128 MiB of HBM per device.

```python
import math
import jax
import jax.numpy as jnp
from jax import lax

D = 2048
HEADS = 16
Q_RANK = 512
KV_RANK = 512
NOPE = 128
ROPE = 64
VDIM = 128
LENGTH = 1024
BATCH = 8


def draw_tokens(key, part):
    value_key = jax.random.fold_in(key, 11)
    values = jnp.clip(jax.random.normal(value_key, (BATCH, LENGTH, D), jnp.float32), -6.0, 6.0)
    return values.astype(jnp.bfloat16)


def base_weight(key, salt, rank, width):
    normal = jax.random.normal(jax.random.fold_in(key, salt), (rank, HEADS, width), jnp.float32)
    return jnp.clip(normal, -4.0, 4.0) * rank ** (-0.5)


def draw_w_qup(key, part):
    values = base_weight(key, 41, Q_RANK, NOPE + ROPE)
    values = jnp.clip(values, -1.0, 1.0)
    return values.reshape(Q_RANK, HEADS * (NOPE + ROPE)).astype(jnp.bfloat16)


def draw_w_kvup(key, part):
    values = base_weight(key, 51, KV_RANK, NOPE + VDIM)
    values = jnp.clip(values, -1.0, 1.0)
    return values.reshape(KV_RANK, HEADS * (NOPE + VDIM)).astype(jnp.bfloat16)


def levels(rng, extent, split, least, largest):
    def one(axis_at, blocks):
        draws = jax.random.uniform(jax.random.fold_in(jax.random.fold_in(rng, 6), axis_at), (blocks,), jnp.float32, least / len(split), largest / len(split))
        return jnp.repeat(jnp.exp(draws), extent[axis_at] // blocks).reshape((-1,) + (1,) * (len(extent) - axis_at - 1))

    level = one(*split[0])
    for cut in split[1:]:
        level = level * one(*cut)
    return level


def centred(stream_key, extent, scale, reach, cuts=(), dtype=jnp.bfloat16):
    factor_of = levels(stream_key, extent, cuts, -0.22, 0.18) if cuts else 1.0
    result = jax.random.normal(stream_key, extent, jnp.float32) * scale * factor_of
    return jnp.minimum(jnp.maximum(result, -reach), reach).astype(dtype)


def setup_inputs(seed: int = 0) -> dict:
    arg_keys = jax.random.split(jax.random.key(seed), 11)
    return {
        "tokens": draw_tokens(jax.random.fold_in(arg_keys[10], 71), 0),
        "w_qdown": centred(arg_keys[1], (D, Q_RANK), D ** -0.5, 0.125, ((0, 8),)),
        "w_kvdown": centred(arg_keys[2], (D, KV_RANK), D ** -0.5, 0.125, ((0, 8),)),
        "w_rotary": centred(arg_keys[3], (D, ROPE), D ** -0.5, 0.125),
        "q_gain": jnp.clip(1.0 + 0.18 * jax.random.normal(arg_keys[4], (Q_RANK,), jnp.float32), 0.1, 1.9),
        "kv_gain": jnp.clip(1.0 + 0.18 * jax.random.normal(arg_keys[5], (KV_RANK,), jnp.float32), 0.1, 1.9),
        "w_qup": draw_w_qup(jax.random.fold_in(arg_keys[10], 71), 0),
        "w_kvup": draw_w_kvup(jax.random.fold_in(arg_keys[10], 71), 0),
        "w_out": centred(arg_keys[8], (HEADS * VDIM, D), (HEADS * VDIM) ** -0.5, 0.125, ((1, 8),)),
        "out_gain": jnp.clip(1.0 + 0.18 * jax.random.normal(arg_keys[9], (D,), jnp.float32), 0.1, 1.9),
    }


EPSILON = 1e-06
THETA = 10000.0

def norm_rows(values, gain):
    scale = lax.rsqrt(lax.optimization_barrier(jnp.mean(values * values, axis=-1, keepdims=True)) + EPSILON)
    return values * scale * gain

def rotate(values, cosine, sine):
    half = values.shape[-1] // 2
    first = values[..., :half]
    second = values[..., half:]
    return jnp.concatenate([first * cosine - second * sine, second * cosine + first * sine], axis=-1)

def reference(tokens, w_qdown, w_kvdown, w_rotary, q_gain, kv_gain, w_qup, w_kvup, w_out, out_gain):
    length = tokens.shape[1]
    positions = jnp.arange(length).astype(jnp.float32)
    freqs = THETA ** (-jnp.arange(0, ROPE, 2).astype(jnp.float32) / ROPE)
    angles = positions[:, None] * freqs[None, :]
    cosine = jnp.cos(angles)
    sine = jnp.sin(angles)
    block = math.gcd(length, 512)
    qk_width = NOPE + ROPE
    scaling = qk_width ** (-0.5)

    def one_sequence(sequence):
        q_lat = jnp.dot(sequence, w_qdown, preferred_element_type=jnp.float32)
        kv_lat = jnp.dot(sequence, w_kvdown, preferred_element_type=jnp.float32)
        q_norm = norm_rows(q_lat, q_gain).astype(jnp.bfloat16)
        kv_norm = norm_rows(kv_lat, kv_gain).astype(jnp.bfloat16)
        key_rot = rotate(jnp.dot(sequence, w_rotary, preferred_element_type=jnp.float32), cosine, sine).astype(jnp.bfloat16)
        q_full = jnp.dot(q_norm, w_qup, preferred_element_type=jnp.float32).reshape(length, HEADS, qk_width)
        q_turn = rotate(q_full[..., NOPE:], cosine[:, None, :], sine[:, None, :])
        queries = jnp.concatenate([q_full[..., :NOPE], q_turn], axis=-1).astype(jnp.bfloat16)
        keyval = jnp.dot(kv_norm, w_kvup, preferred_element_type=jnp.float32).astype(jnp.bfloat16)
        keyval = keyval.reshape(length, HEADS, NOPE + VDIM)
        keys_all = keyval[..., :NOPE].astype(jnp.float32)
        values_all = keyval[..., NOPE:].astype(jnp.float32)
        rot_all = key_rot.astype(jnp.float32)
        outputs = []
        for begin in range(0, length, block):
            finish = begin + block
            query_block = queries[begin:finish].astype(jnp.float32)
            scores = jnp.einsum('qhd,khd->hqk', query_block[..., :NOPE], keys_all[:finish])
            scores = scores + jnp.einsum('qhd,kd->hqk', query_block[..., NOPE:], rot_all[:finish])
            scores = scores * scaling
            query_pos = begin + jnp.arange(block)
            key_pos = jnp.arange(finish)
            allowed = key_pos[None, :] <= query_pos[:, None]
            scores = jnp.where(allowed[None], scores, -jnp.inf)
            top = lax.optimization_barrier(jnp.max(scores, axis=-1, keepdims=True))
            expo = jnp.exp(scores - top)
            weights = (expo / lax.optimization_barrier(jnp.sum(expo, axis=-1, keepdims=True))).astype(jnp.bfloat16)
            attended = jnp.einsum('hqk,khd->qhd', weights.astype(jnp.float32), values_all[:finish])
            outputs.append(attended.astype(jnp.bfloat16))
        attended_all = jnp.concatenate(outputs, axis=0).reshape(length, HEADS * VDIM)
        proj = jnp.dot(attended_all, w_out, preferred_element_type=jnp.float32)
        return norm_rows(proj, out_gain).astype(jnp.bfloat16)
    return lax.map(one_sequence, tokens)
```

```python
import functools
import math

import jax
import jax.numpy as jnp
import numpy as np
from jax import lax
from jax.experimental import pallas as pl
from jax.experimental.pallas import tpu as pltpu
from jax.sharding import PartitionSpec as P

HEADS = 16
NOPE = 128
ROPE = 64
VDIM = 128


EPSILON = 1e-06
THETA = 10000.0
LANES = 128
SUBLANES = 16
MESH = pl.DeviceIdType.MESH


def norm_rows(values, gain):
    scale = lax.rsqrt(jnp.mean(values * values, axis=-1, keepdims=True) + EPSILON)
    return values * scale * gain


def rotate(values, cosine, sine):
    half = values.shape[-1] // 2
    first = values[..., :half]
    second = values[..., half:]
    return jnp.concatenate(
        [first * cosine - second * sine, second * cosine + first * sine], axis=-1
    )


def turn_tables(offset, count):
    positions = (offset + jnp.arange(count)).astype(jnp.float32)
    freqs = THETA ** (-jnp.arange(0, ROPE, 2).astype(jnp.float32) / ROPE)
    angles = positions[:, None] * freqs[None, :]
    return (jnp.cos(angles), jnp.sin(angles))


def make_queries(q_full, cosine, sine, heads_here):
    rows = q_full.shape[0]
    shaped = q_full.reshape(rows, heads_here, NOPE + ROPE)
    turned = rotate(shaped[..., NOPE:], cosine[:, None, :], sine[:, None, :])
    joined = jnp.concatenate([shaped[..., :NOPE], turned], axis=-1)
    return joined.reshape(rows, heads_here * (NOPE + ROPE)).astype(jnp.bfloat16)


def attend(query_heads, keyval_heads, key_rot, heads_here):
    length = query_heads.shape[0]
    block = math.gcd(length, 512)
    scaling = (NOPE + ROPE) ** (-0.5)
    queries = query_heads.reshape(length, heads_here, NOPE + ROPE)
    keyval = keyval_heads.reshape(length, heads_here, NOPE + VDIM)
    keys_all = keyval[..., :NOPE]
    values_all = keyval[..., NOPE:]
    outputs = []
    for begin in range(0, length, block):
        finish = begin + block
        query_block = queries[begin:finish]
        scores = jnp.einsum(
            "qhd,khd->hqk",
            query_block[..., :NOPE],
            keys_all[:finish],
            preferred_element_type=jnp.float32,
        )
        scores = scores + jnp.einsum(
            "qhd,kd->hqk",
            query_block[..., NOPE:],
            key_rot[:finish],
            preferred_element_type=jnp.float32,
        )
        scores = scores * scaling
        query_pos = begin + jnp.arange(block)
        key_pos = jnp.arange(finish)
        allowed = key_pos[None, :] <= query_pos[:, None]
        scores = jnp.where(allowed[None], scores, -jnp.inf)
        top = jnp.max(scores, axis=-1, keepdims=True)
        expo = jnp.exp(scores - top)
        weights = (expo / jnp.sum(expo, axis=-1, keepdims=True)).astype(jnp.bfloat16)
        attended = jnp.einsum(
            "hqk,khd->qhd", weights, values_all[:finish], preferred_element_type=jnp.float32
        )
        outputs.append(attended.astype(jnp.bfloat16))
    return jnp.concatenate(outputs, axis=0).reshape(length, heads_here * VDIM)


def plain_body(tokens, w_qdown, w_kvdown, w_rotary, q_gain, kv_gain, w_qup, w_kvup, w_out, out_gain):
    own_rows = tokens[0]
    tok_count = own_rows.shape[0]
    sp_count = lax.axis_size("sp")
    sp_place = lax.axis_index("sp")
    length = tok_count * sp_count
    heads_here = HEADS // sp_count
    pieces = (
        lax.all_gather(w_qdown, "dp", axis=0, tiled=True),
        lax.all_gather(w_kvdown, "dp", axis=0, tiled=True),
    )
    q_lat = jnp.dot(own_rows, pieces[0], preferred_element_type=jnp.float32)
    kv_lat = jnp.dot(own_rows, pieces[1], preferred_element_type=jnp.float32)
    q_norm = norm_rows(q_lat, q_gain).astype(jnp.bfloat16)
    kv_norm = norm_rows(kv_lat, kv_gain).astype(jnp.bfloat16)
    own_cos, own_sin = turn_tables(sp_place * tok_count, tok_count)
    key_rot = rotate(
        jnp.dot(own_rows, w_rotary, preferred_element_type=jnp.float32), own_cos, own_sin
    ).astype(jnp.bfloat16)
    q_all, kv_all, rot_all = (
        lax.all_gather(q_norm, "sp", axis=0, tiled=True),
        lax.all_gather(kv_norm, "sp", axis=0, tiled=True),
        lax.all_gather(key_rot, "sp", axis=0, tiled=True),
    )
    q_width = heads_here * (NOPE + ROPE)
    kv_width = heads_here * (NOPE + VDIM)
    q_columns = lax.dynamic_slice_in_dim(w_qup, sp_place * q_width, q_width, 1)
    kv_columns = lax.dynamic_slice_in_dim(w_kvup, sp_place * kv_width, kv_width, 1)
    pieces = (
        lax.all_gather(q_columns, "dp", axis=0, tiled=True),
        lax.all_gather(kv_columns, "dp", axis=0, tiled=True),
    )
    q_full = jnp.dot(q_all, pieces[0], preferred_element_type=jnp.float32)
    kv_full = jnp.dot(kv_all, pieces[1], preferred_element_type=jnp.float32)
    all_cos, all_sin = turn_tables(0, length)
    query_heads = make_queries(q_full, all_cos, all_sin, heads_here)
    keyval_heads = kv_full.astype(jnp.bfloat16)
    attended = attend(query_heads, keyval_heads, rot_all, heads_here)
    merged = lax.all_to_all(attended, "sp", split_axis=0, concat_axis=1, tiled=True)
    proj = jnp.dot(
        merged, lax.all_gather(w_out, "dp", axis=1, tiled=True), preferred_element_type=jnp.float32
    )
    mixed = norm_rows(proj, out_gain).astype(jnp.bfloat16)
    return mixed[None]


def turn_table(length):
    positions = np.arange(length, dtype=np.float32)
    freqs = np.float32(THETA) ** (-np.arange(0, ROPE, 2).astype(np.float32) / np.float32(ROPE))
    angles = positions[:, None] * freqs[None, :].astype(np.float32)
    cosine, sine = np.cos(angles), np.sin(angles)
    return np.concatenate([cosine, cosine, sine, sine], axis=1).astype(np.float32)


class Copies:
    def __init__(self, send_sems, recv_sems):
        self.send_sems, self.recv_sems = send_sems, recv_sems
        self.sends = self.receives = 0
        self.sent = []

    def reserve(self, count):
        at = self.receives
        self.receives += count
        assert self.receives <= self.recv_sems.shape[0]
        return at

    def describe(self, source, target, device, send_at, recv_at):
        return pltpu.make_async_remote_copy(
            src_ref=source(),
            dst_ref=target(),
            send_sem=self.send_sems.at[send_at],
            recv_sem=self.recv_sems.at[recv_at],
            device_id=device,
            device_id_type=MESH,
        )

    def start(self, source, target, device, recv_at=None, when=None):
        send_at = self.sends
        self.sends += 1
        assert self.sends <= self.send_sems.shape[0]
        if recv_at is None:
            recv_at = self.reserve(1)

        def make():
            return self.describe(source, target, device, send_at, recv_at)

        guarded(when, lambda: make().start())
        self.sent.append((make, when))
        return lambda: make().wait_recv()

    def drain(self):
        for make, when in self.sent:
            guarded(when, lambda: make().wait_send())


def guarded(when, action):
    if when is None:
        action()
    else:

        @pl.when(when)
        def _():
            action()


class Chain:
    def __init__(self, copies, place, own, view):
        self.copies, self.place, self.own, self.view = copies, place, own, view
        self.arrived = copies.reserve(place["z_count"])

    def start(self):
        place = self.place
        for step in (1, -1):
            near = place["z"] + step
            self.copies.start(
                self.own,
                functools.partial(self.view, place["dp"]),
                {"dp": 2 * near + place["side"]},
                recv_at=self.arrived + place["z"],
                when=place["above"] if step > 0 else place["below"],
            )

    def arrive(self, step):
        place = self.place
        source, slot = place["order"][step], place["slots"][step]
        block = functools.partial(self.view, slot)
        self.copies.describe(
            block, block, {"dp": place["core"]}, 0, self.arrived + source
        ).wait_recv()
        for way in (1, -1):
            onward = place["z"] + way
            coming = source < place["z"] if way > 0 else source > place["z"]
            self.copies.start(
                block,
                block,
                {"dp": 2 * onward + place["side"]},
                recv_at=self.arrived + source,
                when=coming & (place["above"] if way > 0 else place["below"]),
            )


class PlaneSpread:
    def __init__(self, copies, place, view, rows, halves):
        self.copies, self.place, self.view, self.rows = copies, place, view, rows
        self.halves = halves

    def start(self, owner, begin, count, towards):
        block = functools.partial(self.view, self.place[owner], begin, count)
        return self.copies.start(block, block, {"sp": self.place[towards]})

    def send(self):
        rows, half = self.rows, self.rows // 2
        if self.halves:
            self.early_x = self.start("me", 0, half, "x")
            self.early_y = self.start("me", half, half, "y")
            self.late_x = self.start("me", half, half, "x")
            self.late_y = self.start("me", 0, half, "y")
        else:
            self.early_x = self.start("me", 0, rows, "x")
            self.early_y = self.start("me", 0, rows, "y")
            self.late_x = self.late_y = None

    def relay(self):
        half = self.rows // 2
        self.early_x()
        self.first = self.start("x", 0, half, "y")
        self.early_y()
        self.second = self.start("y", half, half, "x")

    def finish_near(self):
        if self.halves:
            self.late_x()
            self.late_y()

    def finish_far(self):
        self.first()
        self.second()


class Gather:
    def __init__(self, copies, place, buffer):
        self.copies, self.place, self.buffer = copies, place, buffer
        self.crossed = []

    def cross(self, source, target):
        self.crossed.append(self.copies.start(source, target, {"dp": self.place["core"]}))

    def finish(self):
        for arrived in self.crossed:
            arrived()


class WeightGather(Gather):
    def __init__(self, copies, place, source, buffer, tail=0, halves=False):
        super().__init__(copies, place, buffer)
        self.source = source
        self.rows = (source.shape[0] - tail) // place["sp_count"]
        self.halves = halves
        self.planes = {}
        start = pl.multiple_of(place["me"] * self.rows, SUBLANES)
        own = lambda: source.at[pl.ds(start, self.rows), :]
        self.chain = Chain(
            copies, place, own, lambda slot: self.piece(slot, place["me"], 0, self.rows)
        )
        if tail:
            rest = pl.ds(source.shape[0] - tail, tail)
            self.tail = lambda slot: buffer.at[slot, rest, :]
            self.tail_chain = Chain(copies, place, lambda: source.at[rest, :], self.tail)

    def piece(self, slot, owner, begin, count):
        start = pl.multiple_of(owner * self.rows + begin, SUBLANES)
        return self.buffer.at[slot, pl.ds(start, count), :]

    def keep(self):
        self.cross(lambda: self.source, lambda: self.buffer.at[self.place["dp"]])

    def cross_piece(self, step, owner):
        slot = self.place["slots"][step]
        block = lambda: self.piece(slot, self.place[owner], 0, self.rows)
        self.cross(block, block)

    def spread(self, step):
        self.chain.arrive(step)
        view = functools.partial(self.piece, self.place["slots"][step])
        plane = PlaneSpread(self.copies, self.place, view, self.rows, self.halves)
        plane.send()
        self.planes[step] = plane
        self.cross_piece(step, "me")

    def relay(self, step):
        self.planes[step].relay()
        if not self.halves:
            self.cross_piece(step, "x")
            self.cross_piece(step, "y")

    def close(self, step):
        self.planes[step].finish_near()
        if self.halves:
            self.cross_piece(step, "x")
            self.cross_piece(step, "y")
        self.planes[step].finish_far()
        self.cross_piece(step, "far")

    def arrive_tail(self, step):
        self.tail_chain.arrive(step)
        slot = self.place["slots"][step]
        block = lambda: self.tail(slot)
        self.cross(block, block)


class ColumnGather(Gather):
    def __init__(self, copies, place, source, buffer):
        super().__init__(copies, place, buffer)
        width = buffer.shape[2]
        start = pl.multiple_of(place["me"] * width, LANES)
        self.own = lambda: source.at[:, pl.ds(start, width)]
        self.view = lambda slot: buffer.at[slot]
        self.chain = Chain(copies, place, self.own, self.view)

    def keep(self):
        self.cross(self.own, lambda: self.buffer.at[self.place["dp"]])

    def arrive(self, step):
        self.chain.arrive(step)
        slot = self.place["slots"][step]
        block = lambda: self.view(slot)
        self.cross(block, block)


def nearest_first(z, z_count, step):
    short = jnp.minimum(z, z_count - 1 - z)
    long_way = jnp.where(2 * z < z_count - 1, 1, -1)
    turn = (step + 1) // 2
    both = z - long_way * turn if step % 2 else z + long_way * turn
    return jnp.where(step <= 2 * short, both, z + long_way * (step - short))


def rotary_picks(rows, offset, skip):
    width = skip + 2 * ROPE
    row = lax.broadcasted_iota(jnp.int32, (rows, width), 0)
    col = lax.broadcasted_iota(jnp.int32, (rows, width), 1)
    half = ROPE // 2
    minus = (col >= skip + ROPE) & (col < skip + ROPE + half)
    origin = jnp.where(
        col < skip + ROPE, col, jnp.where(minus, col - half, col - ROPE - half)
    )
    sign = jnp.where(minus, -1.0, 1.0)
    return jnp.where(row == origin + offset, sign, 0.0).astype(jnp.bfloat16)


def turned(values, table):
    product = values * table
    return product + pltpu.roll(product, ROPE, axis=1)


def dot(left, right):
    return jnp.dot(left, right, preferred_element_type=jnp.float32)


def kernel(
    sp_count, dp_count,
    tokens, w_qdown, w_kvdown, w_rotary, q_gain, kv_gain, w_qup, w_kvup, w_out, out_gain, table,
    out,
    qd_all, kvd_all, qu_all, kvu_all, wo_all, q_lat, kv_lat,
    q_heads, k_heads, v_heads, qu_laid, attended, merged, proj,
    send_sems, recv_sems, back_send, back_recv, local_sems,
):
    scope = jax.named_scope
    me = lax.axis_index("sp")
    dp = lax.axis_index("dp")
    z_count = dp_count // 2
    side = lax.rem(dp, 2)
    z = dp // 2
    steps = range(1, z_count)
    order = {step: nearest_first(z, z_count, step) for step in steps}
    place = {
        "me": me,
        "dp": dp,
        "z": z,
        "side": side,
        "above": z < z_count - 1,
        "below": z > 0,
        "order": order,
        "slots": {step: 2 * order[step] + side for step in steps},
        "sp_count": sp_count,
        "dp_count": dp_count,
        "z_count": z_count,
        "x": me + 1 - 2 * lax.rem(me, 2),
        "y": lax.rem(me + 2, sp_count),
        "far": sp_count - 1 - me,
        "core": dp + 1 - 2 * side,
    }
    count = tokens.shape[0]
    heads = q_heads.shape[0]
    rank = kvd_all.shape[2]

    barrier = pltpu.get_barrier_semaphore()

    def greet(peer):
        pl.semaphore_signal(barrier, inc=1, device_id=peer, device_id_type=MESH)

    for step in range(1, sp_count):
        greet({"sp": lax.rem(me + step, sp_count)})
    greet({"dp": place["core"]})
    guarded(place["above"], lambda: greet({"dp": dp + 2}))
    guarded(place["below"], lambda: greet({"dp": dp - 2}))

    copies = Copies(send_sems, recv_sems)
    kvd = WeightGather(copies, place, w_kvdown, kvd_all)
    qd = WeightGather(copies, place, w_qdown, qd_all)
    kvu = ColumnGather(copies, place, w_kvup, kvu_all)
    qu = ColumnGather(copies, place, w_qup, qu_all)
    wo = WeightGather(copies, place, w_out, wo_all, w_out.shape[0] * 3 // 8, halves=True)
    kept = [
        pltpu.make_async_copy(kvu.own(), kvu_all.at[dp], local_sems.at[0]),
        pltpu.make_async_copy(qu.own(), qu_all.at[dp], local_sems.at[1]),
        pltpu.make_async_copy(w_out, wo_all.at[dp], local_sems.at[2]),
    ]
    for copy in kept:
        copy.start()
    kvd_all[dp] = w_kvdown[...]
    qd_all[dp] = w_qdown[...]

    with scope("barrier"):
        neighbours = place["above"].astype(jnp.int32) + place["below"].astype(jnp.int32)
        pl.semaphore_wait(barrier, sp_count + neighbours)

    kvd.chain.start()
    qd.chain.start()
    for gather in (kvd, qd, kvu, qu, wo):
        gather.keep()

    with scope("keyrot"):
        own_table = table[pl.ds(pl.multiple_of(me * count, SUBLANES), count), :]
        picks = rotary_picks(ROPE, 0, 0)
        rotary = lax.dot_general(
            picks, w_rotary[...], (((0,), (0,)), ((), ())), preferred_element_type=jnp.float32
        ).astype(jnp.bfloat16)
        key_rot = lax.dot_general(
            tokens[...], rotary, (((1,), (1,)), ((), ())), preferred_element_type=jnp.float32
        )
        key_rot = turned(key_rot, own_table)
        lane = lax.broadcasted_iota(jnp.int32, key_rot.shape, 1)
        key_rot = jnp.where(lane < ROPE, key_rot, 0.0).astype(jnp.bfloat16)
        kv_lat[me, :, rank:] = key_rot

    last = steps[-1]
    with scope("kvd_spread"):
        for step in steps:
            kvd.spread(step)
            if step > 1:
                kvd.relay(step - 1)
    kvu.chain.start()
    qu.chain.start()
    with scope("qd_spread"):
        for step in steps:
            qd.spread(step)
            if step > 1:
                qd.relay(step - 1)
            else:
                kvd.relay(last)
    wo.chain.start()
    with scope("kvd_close"):
        for step in steps:
            kvd.close(step)
    with scope("qd_relay"):
        qd.relay(last)
    with scope("kvd_finish"):
        kvd.finish()
    with scope("kv_lat"):
        down = kvd_all[...].reshape(-1, rank)
        kv_lat[me, :, :rank] = norm_rows(dot(tokens[...], down), kv_gain[...]).astype(jnp.bfloat16)

    def block_view(buffer, owner, begin, rows):
        return buffer.at[owner, pl.ds(begin, rows), :]

    kv_plane = PlaneSpread(copies, place, functools.partial(block_view, kv_lat), count, True)
    q_plane = PlaneSpread(copies, place, functools.partial(block_view, q_lat), count, True)
    kv_plane.send()
    with scope("up_arrive"):
        for step in steps[:-1]:
            kvu.arrive(step)
            qu.arrive(step)
    with scope("qd_close"):
        for step in steps:
            qd.close(step)
        qd.finish()
    with scope("q_lat"):
        down = qd_all[...].reshape(-1, qd_all.shape[2])
        q_lat[me] = norm_rows(dot(tokens[...], down), q_gain[...]).astype(jnp.bfloat16)
    with scope("kv_relay"):
        kv_plane.relay()
    q_plane.send()
    with scope("up_last"):
        kvu.arrive(last)
        qu.arrive(last)
    wo.tail_chain.start()
    with scope("wo_spread1"):
        wo.spread(1)
    with scope("q_relay"):
        q_plane.relay()
    with scope("qu_wait"):
        kept[1].wait()
        qu.finish()
    with scope("qu_lay"):
        laid = qu_all[...].reshape(-1, qu_all.shape[2])
        head_width = NOPE + 2 * ROPE
        for head in range(heads):
            picks = rotary_picks(laid.shape[1], head * (NOPE + ROPE), NOPE)
            qu_laid[:, head * head_width : (head + 1) * head_width] = dot(laid, picks).astype(
                jnp.bfloat16
            )
    with scope("wo_relay1"):
        wo.relay(1)
    with scope("kvu_wait"):
        kept[0].wait()
        kvu.finish()
        kv_plane.finish_near()
        kv_plane.finish_far()

    def make_keys(block, _):
        rows = pl.ds(pl.multiple_of(block * count, SUBLANES), count)
        latent = kv_lat[block]
        full = dot(latent[:, :rank], kvu_all[...].reshape(rank, -1)).astype(jnp.bfloat16)
        for head in range(heads):
            at = head * (NOPE + VDIM)
            k_heads[head, rows, :NOPE] = full[:, at : at + NOPE]
            k_heads[head, rows, NOPE:] = latent[:, rank:]
            v_heads[head, rows, :] = full[:, at + NOPE : at + NOPE + VDIM]
        return 0

    with scope("make_keys"):
        lax.fori_loop(0, sp_count, make_keys, 0)
    with scope("wo_spread2"):
        wo.spread(2)
    with scope("q_wait"):
        q_plane.finish_near()
        q_plane.finish_far()

    def make_block(block, _):
        rows = pl.ds(pl.multiple_of(block * count, SUBLANES), count)
        full = dot(q_lat[block], qu_laid[...])
        turns = table[rows, :]
        for head in range(heads):
            at = head * head_width
            q_heads[head, rows, :NOPE] = full[:, at : at + NOPE].astype(jnp.bfloat16)
            part = full[:, at + NOPE : at + head_width]
            q_heads[head, rows, NOPE:] = turned(part, turns).astype(jnp.bfloat16)
        return 0

    with scope("make_q"):
        lax.fori_loop(0, sp_count, make_block, 0)

    factor = (NOPE + ROPE) ** (-0.5) * math.log2(math.e)
    contract = (((1,), (1,)), ((), ()))
    width = heads * VDIM

    def head_lanes(owner, head):
        return pl.ds(pl.multiple_of(owner * width + head * VDIM, LANES), VDIM)

    def back(block, head, source):
        return pltpu.make_async_remote_copy(
            src_ref=attended.at[block, :, head_lanes(0, head)],
            dst_ref=merged.at[:, head_lanes(source, head)],
            send_sem=back_send.at[head, block],
            recv_sem=back_recv.at[head, source],
            device_id={"sp": block},
            device_id_type=MESH,
        )

    def one_head(head, _):
        for block in reversed(range(sp_count)):
            begin = block * count
            query = q_heads[head, begin : begin + count, :]
            near = lax.dot_general(
                query, k_heads[head, begin : begin + count, :], contract,
                preferred_element_type=jnp.float32,
            )
            row = lax.broadcasted_iota(jnp.int32, near.shape, 0)
            col = lax.broadcasted_iota(jnp.int32, near.shape, 1)
            near = jnp.where(col <= row, near, -jnp.inf)
            top = jnp.max(near, axis=-1, keepdims=True)
            if block:
                far = lax.dot_general(
                    query, k_heads[head, :begin, :], contract, preferred_element_type=jnp.float32
                )
                top = jnp.maximum(top, jnp.max(far, axis=-1, keepdims=True))
            near = jnp.exp2((near - top) * factor)
            total = jnp.sum(near, axis=-1, keepdims=True)
            if block:
                far = jnp.exp2((far - top) * factor)
                total = total + jnp.sum(far, axis=-1, keepdims=True)
            share = 1.0 / total
            result = dot((near * share).astype(jnp.bfloat16), v_heads[head, begin : begin + count, :])
            if block:
                result = result + dot((far * share).astype(jnp.bfloat16), v_heads[head, :begin, :])
            attended[block, :, head_lanes(0, head)] = result.astype(jnp.bfloat16)
        for block in range(sp_count):

            @pl.when(me != block)
            def _():
                back(block, head, me).start()

        merged[:, head_lanes(me, head)] = attended[me, :, head_lanes(0, head)]
        return 0

    chores = [[] for _ in range(heads)]
    plan = [functools.partial(wo.spread, step) for step in steps if step > 2]
    plan += [functools.partial(wo.relay, step) for step in steps if step > 1]
    plan += [functools.partial(wo.arrive_tail, step) for step in steps]
    for at, chore in enumerate(plan):
        chores[at * heads // len(plan)].append(chore)
    for head in range(heads):
        with scope("attn"):
            lax.fori_loop(head, head + 1, one_head, 0)
        with scope("chores"):
            for chore in chores[head]:
                chore()

    with scope("wo_wait"):
        for step in steps:
            wo.close(step)
        kept[2].wait()
        wo.finish()
    with scope("a2a_wait"):
        for source in range(sp_count):

            @pl.when(me != source)
            def _():
                for head in range(heads):
                    back(source, head, source).wait()

    out_width = wo_all.shape[2]

    def project(piece, squares):
        lanes = pl.ds(pl.multiple_of(piece * out_width, LANES), out_width)
        value = dot(merged[...], wo_all[piece])
        proj[:, lanes] = value
        return squares + jnp.sum(value * value, axis=-1, keepdims=True)

    with scope("project"):
        squares = lax.fori_loop(0, dp_count, project, jnp.zeros((count, 1), jnp.float32))
        scale = lax.rsqrt(squares * (1.0 / out.shape[1]) + EPSILON)
        out[...] = (proj[...] * scale * out_gain[...]).astype(out.dtype)
    with scope("drain"):
        copies.drain()


def kernel_body(mesh, tokens, w_qdown, w_kvdown, w_rotary, q_gain, kv_gain, w_qup, w_kvup, w_out, out_gain):
    sp_count, dp_count = mesh.shape["sp"], mesh.shape["dp"]
    heads = HEADS // sp_count
    count, depth = tokens.shape[1:]
    length = count * sp_count
    q_rank, kv_rank = w_qdown.shape[1], w_kvdown.shape[1]
    bf16 = jnp.bfloat16
    steps = dp_count // 2 - 1
    sems = 50 * steps + 30
    vmem, hbm = pl.BlockSpec(memory_space=pltpu.VMEM), pl.BlockSpec(memory_space=pl.ANY)
    sp_width = HEADS // sp_count
    mixed = pl.pallas_call(
        functools.partial(kernel, sp_count, dp_count),
        out_shape=jax.ShapeDtypeStruct((count, w_out.shape[1] * dp_count), bf16),
        in_specs=[vmem] * 6 + [hbm] * 3 + [vmem] * 2,
        out_specs=vmem,
        scratch_shapes=[
            pltpu.VMEM((dp_count,) + w_qdown.shape, bf16),
            pltpu.VMEM((dp_count,) + w_kvdown.shape, bf16),
            pltpu.VMEM((dp_count, w_qup.shape[0], sp_width * (NOPE + ROPE)), bf16),
            pltpu.VMEM((dp_count, w_kvup.shape[0], sp_width * (NOPE + VDIM)), bf16),
            pltpu.VMEM((dp_count,) + w_out.shape, bf16),
            pltpu.VMEM((sp_count, count, q_rank), bf16),
            pltpu.VMEM((sp_count, count, kv_rank + 2 * ROPE), bf16),
            pltpu.VMEM((heads, length, NOPE + 2 * ROPE), bf16),
            pltpu.VMEM((heads, length, NOPE + 2 * ROPE), bf16),
            pltpu.VMEM((heads, length, VDIM), bf16),
            pltpu.VMEM((q_rank, heads * (NOPE + 2 * ROPE)), bf16),
            pltpu.VMEM((sp_count, count, heads * VDIM), bf16),
            pltpu.VMEM((count, HEADS * VDIM), bf16),
            pltpu.VMEM((count, w_out.shape[1] * dp_count), jnp.float32),
            pltpu.SemaphoreType.DMA((sems,)),
            pltpu.SemaphoreType.DMA((sems,)),
            pltpu.SemaphoreType.DMA((heads, sp_count)),
            pltpu.SemaphoreType.DMA((heads, sp_count)),
            pltpu.SemaphoreType.DMA((3,)),
        ],
        compiler_params=pltpu.CompilerParams(
            collective_id=0, has_side_effects=True, vmem_limit_bytes=60 * 1024 * 1024
        ),
        name="latent_attention",
    )(
        tokens[0], w_qdown, w_kvdown, w_rotary.T, q_gain[None], kv_gain[None], w_qup, w_kvup, w_out,
        out_gain[None], jnp.asarray(turn_table(length)),
    )
    return mixed[None]


def fits_kernel(mesh):
    return mesh.shape["sp"] == 2 * 2 and mesh.shape["dp"] % 2 == 0


def solution(mesh):
    in_specs = (
        P("dp", "sp", None),
        P("dp", None),
        P("dp", None),
        P(),
        P(),
        P(),
        P("dp", None),
        P("dp", None),
        P(None, "dp"),
        P(),
    )
    out_specs = P("dp", "sp", None)
    body = functools.partial(kernel_body, mesh) if fits_kernel(mesh) else plain_body
    return jax.shard_map(body, mesh=mesh, in_specs=in_specs, out_specs=out_specs, check_vma=False)
```

```python
import functools
import math

import jax
import jax.numpy as jnp
import numpy as np
from jax import lax
from jax.experimental import pallas as pl
from jax.experimental.pallas import tpu as pltpu
from jax.sharding import PartitionSpec as P

HEADS = 16
NOPE = 128
ROPE = 64
VDIM = 128


EPSILON = 1e-06
THETA = 10000.0
LANES = 128
SUBLANES = 16
CHUNKS = 2
MESH = pl.DeviceIdType.MESH


def norm_rows(values, gain):
    scale = lax.rsqrt(jnp.mean(values * values, axis=-1, keepdims=True) + EPSILON)
    return values * scale * gain


def rotate(values, cosine, sine):
    half = values.shape[-1] // 2
    first = values[..., :half]
    second = values[..., half:]
    return jnp.concatenate(
        [first * cosine - second * sine, second * cosine + first * sine], axis=-1
    )


def turn_tables(offset, count):
    positions = (offset + jnp.arange(count)).astype(jnp.float32)
    freqs = THETA ** (-jnp.arange(0, ROPE, 2).astype(jnp.float32) / ROPE)
    angles = positions[:, None] * freqs[None, :]
    return (jnp.cos(angles), jnp.sin(angles))


def make_queries(q_full, cosine, sine, heads_here):
    rows = q_full.shape[0]
    shaped = q_full.reshape(rows, heads_here, NOPE + ROPE)
    turned = rotate(shaped[..., NOPE:], cosine[:, None, :], sine[:, None, :])
    joined = jnp.concatenate([shaped[..., :NOPE], turned], axis=-1)
    return joined.reshape(rows, heads_here * (NOPE + ROPE)).astype(jnp.bfloat16)


def attend(query_heads, keyval_heads, key_rot, heads_here):
    length = query_heads.shape[0]
    block = math.gcd(length, 512)
    scaling = (NOPE + ROPE) ** (-0.5)
    queries = query_heads.reshape(length, heads_here, NOPE + ROPE)
    keyval = keyval_heads.reshape(length, heads_here, NOPE + VDIM)
    keys_all = keyval[..., :NOPE]
    values_all = keyval[..., NOPE:]
    outputs = []
    for begin in range(0, length, block):
        finish = begin + block
        query_block = queries[begin:finish]
        scores = jnp.einsum(
            "qhd,khd->hqk",
            query_block[..., :NOPE],
            keys_all[:finish],
            preferred_element_type=jnp.float32,
        )
        scores = scores + jnp.einsum(
            "qhd,kd->hqk",
            query_block[..., NOPE:],
            key_rot[:finish],
            preferred_element_type=jnp.float32,
        )
        scores = scores * scaling
        query_pos = begin + jnp.arange(block)
        key_pos = jnp.arange(finish)
        allowed = key_pos[None, :] <= query_pos[:, None]
        scores = jnp.where(allowed[None], scores, -jnp.inf)
        top = jnp.max(scores, axis=-1, keepdims=True)
        expo = jnp.exp(scores - top)
        weights = (expo / jnp.sum(expo, axis=-1, keepdims=True)).astype(jnp.bfloat16)
        attended = jnp.einsum(
            "hqk,khd->qhd", weights, values_all[:finish], preferred_element_type=jnp.float32
        )
        outputs.append(attended.astype(jnp.bfloat16))
    return jnp.concatenate(outputs, axis=0).reshape(length, heads_here * VDIM)


def plain_body(tokens, w_qdown, w_kvdown, w_rotary, q_gain, kv_gain, w_qup, w_kvup, w_out, out_gain):
    own_rows = tokens[0]
    tok_count = own_rows.shape[0]
    sp_count = lax.axis_size("sp")
    sp_place = lax.axis_index("sp")
    length = tok_count * sp_count
    heads_here = HEADS // sp_count
    pieces = (
        lax.all_gather(w_qdown, "dp", axis=0, tiled=True),
        lax.all_gather(w_kvdown, "dp", axis=0, tiled=True),
    )
    q_lat = jnp.dot(own_rows, pieces[0], preferred_element_type=jnp.float32)
    kv_lat = jnp.dot(own_rows, pieces[1], preferred_element_type=jnp.float32)
    q_norm = norm_rows(q_lat, q_gain).astype(jnp.bfloat16)
    kv_norm = norm_rows(kv_lat, kv_gain).astype(jnp.bfloat16)
    own_cos, own_sin = turn_tables(sp_place * tok_count, tok_count)
    key_rot = rotate(
        jnp.dot(own_rows, w_rotary, preferred_element_type=jnp.float32), own_cos, own_sin
    ).astype(jnp.bfloat16)
    q_all, kv_all, rot_all = (
        lax.all_gather(q_norm, "sp", axis=0, tiled=True),
        lax.all_gather(kv_norm, "sp", axis=0, tiled=True),
        lax.all_gather(key_rot, "sp", axis=0, tiled=True),
    )
    q_width = heads_here * (NOPE + ROPE)
    kv_width = heads_here * (NOPE + VDIM)
    q_columns = lax.dynamic_slice_in_dim(w_qup, sp_place * q_width, q_width, 1)
    kv_columns = lax.dynamic_slice_in_dim(w_kvup, sp_place * kv_width, kv_width, 1)
    pieces = (
        lax.all_gather(q_columns, "dp", axis=0, tiled=True),
        lax.all_gather(kv_columns, "dp", axis=0, tiled=True),
    )
    q_full = jnp.dot(q_all, pieces[0], preferred_element_type=jnp.float32)
    kv_full = jnp.dot(kv_all, pieces[1], preferred_element_type=jnp.float32)
    all_cos, all_sin = turn_tables(0, length)
    query_heads = make_queries(q_full, all_cos, all_sin, heads_here)
    keyval_heads = kv_full.astype(jnp.bfloat16)
    attended = attend(query_heads, keyval_heads, rot_all, heads_here)
    merged = lax.all_to_all(attended, "sp", split_axis=0, concat_axis=1, tiled=True)
    proj = jnp.dot(
        merged, lax.all_gather(w_out, "dp", axis=1, tiled=True), preferred_element_type=jnp.float32
    )
    mixed = norm_rows(proj, out_gain).astype(jnp.bfloat16)
    return mixed[None]


def turn_table(length):
    positions = np.arange(length, dtype=np.float32)
    freqs = np.float32(THETA) ** (-np.arange(0, ROPE, 2).astype(np.float32) / np.float32(ROPE))
    angles = positions[:, None] * freqs[None, :].astype(np.float32)
    cosine, sine = np.cos(angles), np.sin(angles)
    return np.concatenate([cosine, cosine, sine, sine], axis=1).astype(np.float32)


class Copies:
    def __init__(self, send_sems, recv_sems):
        self.send_sems, self.recv_sems = send_sems, recv_sems
        self.sends = self.receives = 0
        self.owed = []

    def reserve(self, count=1):
        at = self.receives
        self.receives += count
        assert self.receives <= self.recv_sems.shape[0]
        return at

    def reserve_send(self, whole, when=None):
        at = self.sends
        self.sends += 1
        assert self.sends <= self.send_sems.shape[0]
        self.owed.append((whole, at, when))
        return at

    def start(self, source, target, device, send_at, recv_at, when=None):
        def make():
            return pltpu.make_async_remote_copy(
                src_ref=source(),
                dst_ref=target(),
                send_sem=self.send_sems.at[send_at],
                recv_sem=self.recv_sems.at[recv_at],
                device_id=device,
                device_id_type=MESH,
            )

        guarded(when, lambda: make().start())

    def wait(self, whole, at):
        pltpu.make_async_copy(whole(), whole(), self.recv_sems.at[at]).wait()

    def drain(self):
        for whole, at, when in self.owed:
            guarded(
                when,
                lambda: pltpu.make_async_copy(whole(), whole(), self.send_sems.at[at]).wait(),
            )


def guarded(when, action):
    if when is None:
        action()
    else:

        @pl.when(when)
        def _():
            action()


class Direct:
    def __init__(self, copies, place, own, view, whole):
        self.copies, self.place, self.own, self.view = copies, place, own, view
        self.arrived = copies.reserve(place["z_count"])
        self.sent = copies.reserve_send(whole)

    def start(self):
        place = self.place
        for step in reversed(place["steps"]):
            self.copies.start(
                self.own,
                functools.partial(self.view, place["dp"]),
                {"dp": place["slots"][step]},
                self.sent,
                self.arrived + place["z"],
            )

    def forward(self, step):
        pass

    def settle(self, step):
        source, slot = self.place["order"][step], self.place["slots"][step]
        self.copies.wait(functools.partial(self.view, slot), self.arrived + source)


class Chain:
    def __init__(self, copies, place, own, view):
        self.copies, self.place, self.own, self.view = copies, place, own, view
        self.arrived = copies.reserve(place["z_count"])

    def start(self):
        place = self.place
        block = functools.partial(self.view, place["dp"])
        for way in (1, -1):
            onward = place["z"] + way
            when = place["above"] if way > 0 else place["below"]
            self.copies.start(
                self.own,
                block,
                {"dp": 2 * onward + place["side"]},
                self.copies.reserve_send(block, when),
                self.arrived + place["z"],
                when,
            )

    def passes(self, step):
        place, source = self.place, self.place["order"][step]
        rising = (source < place["z"]) & place["above"]
        sinking = (source > place["z"]) & place["below"]
        return rising, sinking

    def block(self, step):
        return functools.partial(self.view, self.place["slots"][step])

    def forward(self, step):
        place = self.place
        source, block = place["order"][step], self.block(step)
        rising, sinking = self.passes(step)
        sent = self.copies.reserve_send(block, rising | sinking)

        def move():
            self.copies.wait(block, self.arrived + source)
            for way in (1, -1):
                onward = place["z"] + way
                self.copies.start(
                    block,
                    block,
                    {"dp": 2 * onward + place["side"]},
                    sent,
                    self.arrived + source,
                    rising if way > 0 else sinking,
                )

        guarded(rising | sinking, move)

    def settle(self, step):
        source, block = self.place["order"][step], self.block(step)
        rising, sinking = self.passes(step)
        guarded(
            jnp.logical_not(rising | sinking),
            lambda: self.copies.wait(block, self.arrived + source),
        )


class PlaneSpread:
    def __init__(self, copies, place, view, span, rows, halves, sent):
        self.copies, self.place, self.view, self.rows = copies, place, view, rows
        self.span, self.halves, self.sent = span, halves, sent
        self.early_x, self.early_y, self.rest = (copies.reserve() for _ in range(3))

    def start(self, owner, begin, count, towards, recv_at):
        block = functools.partial(self.view, self.place[owner], begin, count)
        self.copies.start(block, block, {"sp": self.place[towards]}, self.sent, recv_at)

    def send(self):
        rows, half = self.rows, self.rows // 2
        if self.halves:
            self.start("me", 0, half, "x", self.early_x)
            self.start("me", half, half, "y", self.early_y)
            self.start("me", half, half, "x", self.rest)
            self.start("me", 0, half, "y", self.rest)
        else:
            self.start("me", 0, rows, "x", self.early_x)
            self.start("me", 0, rows, "y", self.early_y)

    def relay(self):
        half = self.rows // 2
        early = half if self.halves else self.rows
        self.copies.wait(functools.partial(self.view, self.place["x"], 0, early), self.early_x)
        self.start("x", 0, half, "y", self.rest)
        begin = half if self.halves else 0
        self.copies.wait(functools.partial(self.view, self.place["y"], begin, early), self.early_y)
        self.start("y", half, half, "x", self.rest)

    def finish(self):
        self.copies.wait(functools.partial(self.span, 4 if self.halves else 2), self.rest)


class Gather:
    def __init__(self, copies, place, buffer, groups):
        self.copies, self.place, self.buffer = copies, place, buffer
        self.crossed = [copies.reserve() for _ in range(groups)]
        self.cross_sent = copies.reserve_send(lambda: buffer.at[pl.ds(0, place["z_count"])])

    def cross(self, step, source, target):
        self.copies.start(
            source,
            target,
            {"dp": self.place["core"]},
            self.cross_sent,
            self.crossed[step % len(self.crossed)],
        )

    def keep(self):
        self.cross(0, self.own_whole, lambda: self.buffer.at[self.place["dp"]])

    def finish(self):
        self.copies.wait(lambda: self.buffer.at[pl.ds(0, self.place["z_count"])], self.crossed[0])

    def finish_step(self, step):
        self.copies.wait(lambda: self.buffer.at[0], self.crossed[step])


class WeightGather(Gather):
    def __init__(self, copies, place, source, buffer, tail=0, chunks=1, chained=False):
        super().__init__(copies, place, buffer, place["z_count"] if chained else 1)
        self.own_whole = (lambda: source) if chained else (lambda: buffer.at[place["dp"]])
        self.rows = (source.shape[0] - tail) // place["sp_count"]
        self.halves = chained
        self.planes = {}
        self.plane_sent = copies.reserve_send(
            lambda: buffer.at[pl.ds(0, len(place["steps"])), pl.ds(0, 3 * self.rows), :]
        )
        start = pl.multiple_of(place["me"] * self.rows, SUBLANES)
        own = lambda: source.at[pl.ds(start, self.rows), :]
        view = lambda slot: self.piece(slot, place["me"], 0, self.rows)
        if chained:
            self.chain = Chain(copies, place, own, view)
        else:
            whole = lambda: source.at[pl.ds(0, self.rows * len(place["steps"])), :]
            self.chain = Direct(copies, place, lambda: view(place["dp"]), view, whole)
        if tail:
            part = tail // chunks
            self.tails = []
            for at in range(source.shape[0] - tail, source.shape[0], part):
                rest = pl.ds(at, part)
                view = lambda slot, rest=rest: buffer.at[slot, rest, :]
                own = lambda rest=rest: source.at[rest, :]
                self.tails.append(Chain(copies, place, own, view))

    def piece(self, slot, owner, begin, count):
        start = pl.multiple_of(owner * self.rows + begin, SUBLANES)
        return self.buffer.at[slot, pl.ds(start, count), :]

    def span(self, halves):
        return self.buffer.at[0, pl.ds(0, halves * (self.rows // 2)), :]

    def cross_piece(self, step, owner):
        slot = self.place["slots"][step]
        block = lambda: self.piece(slot, self.place[owner], 0, self.rows)
        self.cross(step, block, block)

    def spread(self, step):
        self.chain.settle(step)
        view = functools.partial(self.piece, self.place["slots"][step])
        plane = PlaneSpread(
            self.copies, self.place, view, self.span, self.rows, self.halves, self.plane_sent
        )
        plane.send()
        self.planes[step] = plane
        self.cross_piece(step, "me")

    def relay(self, step):
        self.planes[step].relay()
        if not self.halves:
            self.cross_piece(step, "x")
            self.cross_piece(step, "y")

    def close(self, step):
        self.planes[step].finish()
        if self.halves:
            self.cross_piece(step, "x")
            self.cross_piece(step, "y")
        self.cross_piece(step, "far")

    def start_tail(self, chunk):
        self.tails[chunk].start()

    def forward_tail(self, chunk, step):
        self.tails[chunk].forward(step)

    def settle_tail(self, chunk, step):
        tail = self.tails[chunk]
        tail.settle(step)
        self.cross(step, tail.block(step), tail.block(step))


class ColumnGather(Gather):
    def __init__(self, copies, place, source, buffer):
        super().__init__(copies, place, buffer, 1)
        width = buffer.shape[2]
        start = pl.multiple_of(place["me"] * width, LANES)
        self.own_whole = lambda: source.at[:, pl.ds(start, width)]
        self.view = lambda slot: buffer.at[slot]
        self.chain = Chain(copies, place, self.own_whole, self.view)

    def settle(self, step):
        self.chain.settle(step)
        slot = self.place["slots"][step]
        block = lambda: self.view(slot)
        self.cross(step, block, block)


def nearest_first(z, z_count, step):
    short = jnp.minimum(z, z_count - 1 - z)
    long_way = jnp.where(2 * z < z_count - 1, 1, -1)
    turn = (step + 1) // 2
    both = z - long_way * turn if step % 2 else z + long_way * turn
    return jnp.where(step <= 2 * short, both, z + long_way * (step - short))


def rotary_picks(rows, offset, skip):
    width = skip + 2 * ROPE
    row = lax.broadcasted_iota(jnp.int32, (rows, width), 0)
    col = lax.broadcasted_iota(jnp.int32, (rows, width), 1)
    half = ROPE // 2
    minus = (col >= skip + ROPE) & (col < skip + ROPE + half)
    origin = jnp.where(
        col < skip + ROPE, col, jnp.where(minus, col - half, col - ROPE - half)
    )
    sign = jnp.where(minus, -1.0, 1.0)
    return jnp.where(row == origin + offset, sign, 0.0).astype(jnp.bfloat16)


def turned(values, table):
    product = values * table
    return product + pltpu.roll(product, ROPE, axis=1)


def dot(left, right):
    return jnp.dot(left, right, preferred_element_type=jnp.float32)


def kernel(
    sp_count, dp_count,
    tokens_in, w_qdown, w_kvdown, rotary_in, q_gain_in, kv_gain_in, w_qup, w_kvup, w_out,
    out_gain_in, table_in,
    out,
    tokens, w_rotary, q_gain, kv_gain, out_gain, table,
    qd_all, kvd_all, qu_all, kvu_all, wo_all, q_lat, kv_lat, rot_all,
    q_heads, k_heads, v_heads, qu_laid, attended, merged, proj,
    send_sems, recv_sems, back_send, back_recv, local_sems,
):
    scope = jax.named_scope
    me = lax.axis_index("sp")
    dp = lax.axis_index("dp")
    z_count = dp_count // 2
    side = lax.rem(dp, 2)
    z = dp // 2
    steps = range(1, z_count)
    order = {step: nearest_first(z, z_count, step) for step in steps}
    place = {
        "me": me,
        "dp": dp,
        "z": z,
        "side": side,
        "above": z < z_count - 1,
        "below": z > 0,
        "order": order,
        "slots": {step: 2 * order[step] + side for step in steps},
        "sp_count": sp_count,
        "dp_count": dp_count,
        "z_count": z_count,
        "steps": steps,
        "x": me + 1 - 2 * lax.rem(me, 2),
        "y": lax.rem(me + 2, sp_count),
        "far": sp_count - 1 - me,
        "core": dp + 1 - 2 * side,
    }
    count = tokens.shape[0]
    heads = q_heads.shape[0]
    rank = kvd_all.shape[2]

    barrier = pltpu.get_barrier_semaphore()

    def greet(peer):
        pl.semaphore_signal(barrier, inc=1, device_id=peer, device_id_type=MESH)

    for step in range(1, sp_count):
        greet({"sp": lax.rem(me + step, sp_count)})
    greet({"dp": place["core"]})
    for step in steps:
        greet({"dp": lax.rem(dp + 2 * step, dp_count)})

    copies = Copies(send_sems, recv_sems)
    kvd = WeightGather(copies, place, w_kvdown, kvd_all)
    qd = WeightGather(copies, place, w_qdown, qd_all)
    kvu = ColumnGather(copies, place, w_kvup, kvu_all)
    qu = ColumnGather(copies, place, w_qup, qu_all)
    wo = WeightGather(copies, place, w_out, wo_all, w_out.shape[0] * 7 // 16, chunks=CHUNKS, chained=True)
    places = [
        (w_kvdown, kvd_all.at[dp]),
        (rotary_in, w_rotary),
        (tokens_in, tokens),
        (table_in, table),
        (w_qdown, qd_all.at[dp]),
        (kv_gain_in, kv_gain),
        (q_gain_in, q_gain),
        (out_gain_in, out_gain),
        (qu.own_whole(), qu_all.at[dp]),
        (kvu.own_whole(), kvu_all.at[dp]),
        (w_out, wo_all.at[dp]),
    ]
    loads = [
        pltpu.make_async_copy(source, target, local_sems.at[at])
        for at, (source, target) in enumerate(places)
    ]
    for load in loads:
        load.start()

    with scope("barrier"):
        pl.semaphore_wait(barrier, sp_count + len(steps))

    loads[0].wait()
    kvd.chain.start()
    kvd.keep()
    for load in loads[1:8]:
        load.wait()
    for gather in (qd, kvu, qu, wo):
        gather.keep()

    with scope("keyrot"):
        own_table = table[pl.ds(pl.multiple_of(me * count, SUBLANES), count), :]
        picks = rotary_picks(ROPE, 0, 0)
        rotary = lax.dot_general(
            picks, w_rotary[...], (((0,), (0,)), ((), ())), preferred_element_type=jnp.float32
        ).astype(jnp.bfloat16)
        key_rot = lax.dot_general(
            tokens[...], rotary, (((1,), (1,)), ((), ())), preferred_element_type=jnp.float32
        )
        key_rot = turned(key_rot, own_table)
        lane = lax.broadcasted_iota(jnp.int32, key_rot.shape, 1)
        rot_all[me] = jnp.where(lane < ROPE, key_rot, 0.0).astype(jnp.bfloat16)

    last = steps[-1]

    def block_view(buffer, owner, begin, rows):
        return buffer.at[owner, pl.ds(begin, rows), :]

    def latent_plane(buffer):
        sent = copies.reserve_send(lambda: buffer.at[pl.ds(0, 3)])
        span = lambda halves: buffer.at[pl.ds(0, halves // 2)]
        view = functools.partial(block_view, buffer)
        return PlaneSpread(copies, place, view, span, count, True, sent)

    rot_plane = latent_plane(rot_all)
    kv_plane = latent_plane(kv_lat)
    q_plane = latent_plane(q_lat)

    def make_kv_latent():
        down = kvd_all[...].reshape(-1, rank)
        kv_lat[me] = norm_rows(dot(tokens[...], down), kv_gain[...]).astype(jnp.bfloat16)

    def make_q_latent():
        down = qd_all[...].reshape(-1, qd_all.shape[2])
        q_lat[me] = norm_rows(dot(tokens[...], down), q_gain[...]).astype(jnp.bfloat16)

    def lay_queries():
        laid = qu_all[...].reshape(-1, qu_all.shape[2])
        for head in range(heads):
            picks = rotary_picks(laid.shape[1], head * (NOPE + ROPE), NOPE)
            qu_laid[:, head * head_width : (head + 1) * head_width] = dot(laid, picks).astype(
                jnp.bfloat16
            )

    head_width = NOPE + 2 * ROPE

    def do(name, action, *args):
        with scope(name + "".join(str(a) for a in args)):
            action(*args)

    def make_keys(block, _):
        rows = pl.ds(pl.multiple_of(block * count, SUBLANES), count)
        latent = kv_lat[block]
        full = dot(latent, kvu_all[...].reshape(rank, -1)).astype(jnp.bfloat16)
        for head in range(heads):
            at = head * (NOPE + VDIM)
            k_heads[head, rows, :NOPE] = full[:, at : at + NOPE]
            k_heads[head, rows, NOPE:] = rot_all[block]
            v_heads[head, rows, :] = full[:, at + NOPE : at + NOPE + VDIM]
        return 0

    def make_all_keys():
        lax.fori_loop(0, sp_count, make_keys, 0)

    def make_block(block, _):
        rows = pl.ds(pl.multiple_of(block * count, SUBLANES), count)
        full = dot(q_lat[block], qu_laid[...])
        turns = table[rows, :]
        for head in range(heads):
            at = head * head_width
            q_heads[head, rows, :NOPE] = full[:, at : at + NOPE].astype(jnp.bfloat16)
            part = full[:, at + NOPE : at + head_width]
            q_heads[head, rows, NOPE:] = turned(part, turns).astype(jnp.bfloat16)
        return 0

    def make_all_queries():
        lax.fori_loop(0, sp_count, make_block, 0)

    factor = (NOPE + ROPE) ** (-0.5) * math.log2(math.e)
    contract = (((1,), (1,)), ((), ()))
    width = heads * VDIM

    def head_lanes(owner, head):
        return pl.ds(pl.multiple_of(owner * width + head * VDIM, LANES), VDIM)

    def back(block, head, source):
        return pltpu.make_async_remote_copy(
            src_ref=attended.at[block, :, head_lanes(0, head)],
            dst_ref=merged.at[:, head_lanes(source, head)],
            send_sem=back_send,
            recv_sem=back_recv,
            device_id={"sp": block},
            device_id_type=MESH,
        )

    def one_head(head, _):
        for block in reversed(range(sp_count)):
            begin = block * count
            query = q_heads[head, begin : begin + count, :]
            near = lax.dot_general(
                query, k_heads[head, begin : begin + count, :], contract,
                preferred_element_type=jnp.float32,
            )
            row = lax.broadcasted_iota(jnp.int32, near.shape, 0)
            col = lax.broadcasted_iota(jnp.int32, near.shape, 1)
            near = jnp.where(col <= row, near, -jnp.inf)
            top = jnp.max(near, axis=-1, keepdims=True)
            if block:
                far = lax.dot_general(
                    query, k_heads[head, :begin, :], contract, preferred_element_type=jnp.float32
                )
                top = jnp.maximum(top, jnp.max(far, axis=-1, keepdims=True))
            near = jnp.exp2((near - top) * factor)
            total = jnp.sum(near, axis=-1, keepdims=True)
            if block:
                far = jnp.exp2((far - top) * factor)
                total = total + jnp.sum(far, axis=-1, keepdims=True)
            share = 1.0 / total
            result = dot((near * share).astype(jnp.bfloat16), v_heads[head, begin : begin + count, :])
            if block:
                result = result + dot((far * share).astype(jnp.bfloat16), v_heads[head, :begin, :])
            attended[block, :, head_lanes(0, head)] = result.astype(jnp.bfloat16)
        for block in range(sp_count):

            @pl.when(me != block)
            def _():
                back(block, head, me).start()

        merged[:, head_lanes(me, head)] = attended[me, :, head_lanes(0, head)]
        return 0

    def attend_head(head):
        lax.fori_loop(head, head + 1, one_head, 0)

    others = attended.at[pl.ds(0, sp_count - 1)]
    out_width = wo_all.shape[2]

    def wait_back():
        pltpu.make_async_copy(others, others, back_recv).wait()

    def project(step, squares):
        with scope(f"project{step}"):
            for core in range(2):
                piece = 2 * (order[step] if step else z) + core
                lanes = pl.ds(pl.multiple_of(piece * out_width, LANES), out_width)
                value = dot(merged[...], wo_all[piece])
                proj[:, lanes] = value
                squares = squares + jnp.sum(value * value, axis=-1, keepdims=True)
        return squares

    rot_plane.send()
    do("kd_s", kvd.spread, 1)
    do("kd_s", kvd.spread, 2)
    qd.chain.start()
    do("rot_r", rot_plane.relay)
    do("kd_r", kvd.relay, 1)
    do("kd_s", kvd.spread, 3)
    kvu.chain.start()
    qu.chain.start()
    wo.chain.start()
    do("kd_r", kvd.relay, 2)
    do("kd_r", kvd.relay, 3)
    do("qd_s", qd.spread, 1)
    do("qd_s", qd.spread, 2)
    do("kd_c", kvd.close, 1)
    do("kd_c", kvd.close, 2)
    do("qd_r", qd.relay, 1)
    do("qd_s", qd.spread, 3)
    do("kd_c", kvd.close, 3)
    do("kvu_fw", kvu.chain.forward, 1)
    do("qu_fw", qu.chain.forward, 1)
    do("kvu_fw", kvu.chain.forward, 2)
    do("qu_fw", qu.chain.forward, 2)
    wo.start_tail(0)
    do("qd_r", qd.relay, 2)
    do("kd_f", kvd.finish)
    do("kv_lat", make_kv_latent)
    kv_plane.send()
    do("qd_r", qd.relay, 3)
    do("qd_c", qd.close, 1)
    do("qd_c", qd.close, 2)
    do("kv_r", kv_plane.relay)
    do("qd_c", qd.close, 3)
    do("qd_f", qd.finish)
    do("q_lat", make_q_latent)
    q_plane.send()
    do("kvu_fw", kvu.chain.forward, 3)
    do("qu_fw", qu.chain.forward, 3)
    do("wo_fw", wo.chain.forward, 1)
    do("wo_fw", wo.chain.forward, 2)
    do("q_r", q_plane.relay)
    do("wo_s", wo.spread, 1)
    do("wo_fw", wo.chain.forward, 3)
    do("t0_fw", wo.forward_tail, 0, 1)
    do("t0_fw", wo.forward_tail, 0, 2)
    wo.start_tail(1)
    do("qu_st", qu.settle, 1)
    do("kvu_st", kvu.settle, 1)
    do("qu_st", qu.settle, 2)
    do("kvu_st", kvu.settle, 2)
    do("qu_st", qu.settle, 3)
    do("kvu_st", kvu.settle, 3)
    loads[9].wait()
    do("kvu_f", kvu.finish)
    do("rot_f", rot_plane.finish)
    do("kv_f", kv_plane.finish)
    do("make_keys", make_all_keys)
    loads[8].wait()
    do("qu_f", qu.finish)
    do("qu_lay", lay_queries)
    do("wo_s", wo.spread, 2)
    do("wo_r", wo.relay, 1)
    do("q_f", q_plane.finish)
    do("make_q", make_all_queries)
    do("t0_fw", wo.forward_tail, 0, 3)
    do("attn", attend_head, 0)
    do("wo_s", wo.spread, 3)
    do("t1_fw", wo.forward_tail, 1, 1)
    do("t1_fw", wo.forward_tail, 1, 2)
    do("attn", attend_head, 1)
    do("wo_r", wo.relay, 2)
    do("attn", attend_head, 2)
    do("t1_fw", wo.forward_tail, 1, 3)
    do("wo_r", wo.relay, 3)
    do("attn", attend_head, 3)
    do("wo_c", wo.close, 1)
    do("t0_st", wo.settle_tail, 0, 1)
    do("t0_st", wo.settle_tail, 0, 2)
    do("t0_st", wo.settle_tail, 0, 3)
    do("t1_st", wo.settle_tail, 1, 1)
    do("t1_st", wo.settle_tail, 1, 2)
    do("wo_c", wo.close, 2)
    do("t1_st", wo.settle_tail, 1, 3)
    do("wo_c", wo.close, 3)
    do("a2a", wait_back)
    squares = jnp.zeros((count, 1), jnp.float32)
    loads[10].wait()
    do("wo_f", wo.finish_step, 0)
    squares = project(0, squares)
    do("wo_f", wo.finish_step, 1)
    squares = project(1, squares)
    do("wo_f", wo.finish_step, 2)
    squares = project(2, squares)
    do("wo_f", wo.finish_step, 3)
    squares = project(3, squares)
    with scope("norm"):
        scale = lax.rsqrt(squares * (1.0 / out.shape[1]) + EPSILON)
        out[...] = (proj[...] * scale * out_gain[...]).astype(out.dtype)
    with scope("drain"):
        copies.drain()
        pltpu.make_async_copy(others, others, back_send).wait()


def kernel_body(mesh, tokens, w_qdown, w_kvdown, w_rotary, q_gain, kv_gain, w_qup, w_kvup, w_out, out_gain):
    sp_count, dp_count = mesh.shape["sp"], mesh.shape["dp"]
    heads = HEADS // sp_count
    count, depth = tokens.shape[1:]
    length = count * sp_count
    q_rank, kv_rank = w_qdown.shape[1], w_kvdown.shape[1]
    bf16 = jnp.bfloat16
    steps = dp_count // 2 - 1
    chains = 3 + CHUNKS
    sends = chains * (steps + 2) + 13
    receives = 3 * 3 * steps + 9 + (chains + 2) * (steps + 1) + 4 + steps + 1
    vmem, hbm = pl.BlockSpec(memory_space=pltpu.VMEM), pl.BlockSpec(memory_space=pl.ANY)
    sp_width = HEADS // sp_count
    mixed = pl.pallas_call(
        functools.partial(kernel, sp_count, dp_count),
        out_shape=pltpu.VMEM((count, w_out.shape[1] * dp_count), bf16),
        in_specs=[hbm] * 11,
        out_specs=vmem,
        scratch_shapes=[
            pltpu.VMEM((count, depth), bf16),
            pltpu.VMEM(w_rotary.shape[::-1], bf16),
            pltpu.VMEM((1, q_rank), jnp.float32),
            pltpu.VMEM((1, kv_rank), jnp.float32),
            pltpu.VMEM((1, out_gain.shape[0]), jnp.float32),
            pltpu.VMEM((length, 4 * (ROPE // 2)), jnp.float32),
            pltpu.VMEM((dp_count,) + w_qdown.shape, bf16),
            pltpu.VMEM((dp_count,) + w_kvdown.shape, bf16),
            pltpu.VMEM((dp_count, w_qup.shape[0], sp_width * (NOPE + ROPE)), bf16),
            pltpu.VMEM((dp_count, w_kvup.shape[0], sp_width * (NOPE + VDIM)), bf16),
            pltpu.VMEM((dp_count,) + w_out.shape, bf16),
            pltpu.VMEM((sp_count, count, q_rank), bf16),
            pltpu.VMEM((sp_count, count, kv_rank), bf16),
            pltpu.VMEM((sp_count, count, 2 * ROPE), bf16),
            pltpu.VMEM((heads, length, NOPE + 2 * ROPE), bf16),
            pltpu.VMEM((heads, length, NOPE + 2 * ROPE), bf16),
            pltpu.VMEM((heads, length, VDIM), bf16),
            pltpu.VMEM((q_rank, heads * (NOPE + 2 * ROPE)), bf16),
            pltpu.VMEM((sp_count, count, heads * VDIM), bf16),
            pltpu.VMEM((count, HEADS * VDIM), bf16),
            pltpu.VMEM((count, w_out.shape[1] * dp_count), jnp.float32),
            pltpu.SemaphoreType.DMA((sends,)),
            pltpu.SemaphoreType.DMA((receives,)),
            pltpu.SemaphoreType.DMA,
            pltpu.SemaphoreType.DMA,
            pltpu.SemaphoreType.DMA((11,)),
        ],
        compiler_params=pltpu.CompilerParams(
            collective_id=0, has_side_effects=True, vmem_limit_bytes=60 * 1024 * 1024
        ),
        name="latent_attention",
    )(
        tokens[0], w_qdown, w_kvdown, w_rotary.T, q_gain[None], kv_gain[None], w_qup, w_kvup, w_out,
        out_gain[None], jnp.asarray(turn_table(length)),
    )
    return mixed[None]


def fits_kernel(mesh):
    return mesh.shape["sp"] == 2 * 2 and mesh.shape["dp"] % 2 == 0


def solution(mesh):
    in_specs = (
        P("dp", "sp", None),
        P("dp", None),
        P("dp", None),
        P(),
        P(),
        P(),
        P("dp", None),
        P("dp", None),
        P(None, "dp"),
        P(),
    )
    out_specs = P("dp", "sp", None)
    body = functools.partial(kernel_body, mesh) if fits_kernel(mesh) else plain_body
    return jax.shard_map(body, mesh=mesh, in_specs=in_specs, out_specs=out_specs, check_vma=False)
```

```python
import functools
import math

import jax
import jax.numpy as jnp
import numpy as np
from jax import lax
from jax.experimental import pallas as pl
from jax.experimental.pallas import tpu as pltpu
from jax.sharding import PartitionSpec as P

HEADS = 16
NOPE = 128
ROPE = 64
VDIM = 128


EPSILON = 1e-06
THETA = 10000.0
LANES = 128
SUBLANES = 16
CHUNKS = 2
MESH = pl.DeviceIdType.MESH


def norm_rows(values, gain):
    scale = lax.rsqrt(jnp.mean(values * values, axis=-1, keepdims=True) + EPSILON)
    return values * scale * gain


def rotate(values, cosine, sine):
    half = values.shape[-1] // 2
    first = values[..., :half]
    second = values[..., half:]
    return jnp.concatenate(
        [first * cosine - second * sine, second * cosine + first * sine], axis=-1
    )


def turn_tables(offset, count):
    positions = (offset + jnp.arange(count)).astype(jnp.float32)
    freqs = THETA ** (-jnp.arange(0, ROPE, 2).astype(jnp.float32) / ROPE)
    angles = positions[:, None] * freqs[None, :]
    return (jnp.cos(angles), jnp.sin(angles))


def make_queries(q_full, cosine, sine, heads_here):
    rows = q_full.shape[0]
    shaped = q_full.reshape(rows, heads_here, NOPE + ROPE)
    turned = rotate(shaped[..., NOPE:], cosine[:, None, :], sine[:, None, :])
    joined = jnp.concatenate([shaped[..., :NOPE], turned], axis=-1)
    return joined.reshape(rows, heads_here * (NOPE + ROPE)).astype(jnp.bfloat16)


def attend(query_heads, keyval_heads, key_rot, heads_here):
    length = query_heads.shape[0]
    block = math.gcd(length, 512)
    scaling = (NOPE + ROPE) ** (-0.5)
    queries = query_heads.reshape(length, heads_here, NOPE + ROPE)
    keyval = keyval_heads.reshape(length, heads_here, NOPE + VDIM)
    keys_all = keyval[..., :NOPE]
    values_all = keyval[..., NOPE:]
    outputs = []
    for begin in range(0, length, block):
        finish = begin + block
        query_block = queries[begin:finish]
        scores = jnp.einsum(
            "qhd,khd->hqk",
            query_block[..., :NOPE],
            keys_all[:finish],
            preferred_element_type=jnp.float32,
        )
        scores = scores + jnp.einsum(
            "qhd,kd->hqk",
            query_block[..., NOPE:],
            key_rot[:finish],
            preferred_element_type=jnp.float32,
        )
        scores = scores * scaling
        query_pos = begin + jnp.arange(block)
        key_pos = jnp.arange(finish)
        allowed = key_pos[None, :] <= query_pos[:, None]
        scores = jnp.where(allowed[None], scores, -jnp.inf)
        top = jnp.max(scores, axis=-1, keepdims=True)
        expo = jnp.exp(scores - top)
        weights = (expo / jnp.sum(expo, axis=-1, keepdims=True)).astype(jnp.bfloat16)
        attended = jnp.einsum(
            "hqk,khd->qhd", weights, values_all[:finish], preferred_element_type=jnp.float32
        )
        outputs.append(attended.astype(jnp.bfloat16))
    return jnp.concatenate(outputs, axis=0).reshape(length, heads_here * VDIM)


def plain_body(tokens, w_qdown, w_kvdown, w_rotary, q_gain, kv_gain, w_qup, w_kvup, w_out, out_gain):
    own_rows = tokens[0]
    tok_count = own_rows.shape[0]
    sp_count = lax.axis_size("sp")
    sp_place = lax.axis_index("sp")
    length = tok_count * sp_count
    heads_here = HEADS // sp_count
    pieces = (
        lax.all_gather(w_qdown, "dp", axis=0, tiled=True),
        lax.all_gather(w_kvdown, "dp", axis=0, tiled=True),
    )
    q_lat = jnp.dot(own_rows, pieces[0], preferred_element_type=jnp.float32)
    kv_lat = jnp.dot(own_rows, pieces[1], preferred_element_type=jnp.float32)
    q_norm = norm_rows(q_lat, q_gain).astype(jnp.bfloat16)
    kv_norm = norm_rows(kv_lat, kv_gain).astype(jnp.bfloat16)
    own_cos, own_sin = turn_tables(sp_place * tok_count, tok_count)
    key_rot = rotate(
        jnp.dot(own_rows, w_rotary, preferred_element_type=jnp.float32), own_cos, own_sin
    ).astype(jnp.bfloat16)
    q_all, kv_all, rot_all = (
        lax.all_gather(q_norm, "sp", axis=0, tiled=True),
        lax.all_gather(kv_norm, "sp", axis=0, tiled=True),
        lax.all_gather(key_rot, "sp", axis=0, tiled=True),
    )
    q_width = heads_here * (NOPE + ROPE)
    kv_width = heads_here * (NOPE + VDIM)
    q_columns = lax.dynamic_slice_in_dim(w_qup, sp_place * q_width, q_width, 1)
    kv_columns = lax.dynamic_slice_in_dim(w_kvup, sp_place * kv_width, kv_width, 1)
    pieces = (
        lax.all_gather(q_columns, "dp", axis=0, tiled=True),
        lax.all_gather(kv_columns, "dp", axis=0, tiled=True),
    )
    q_full = jnp.dot(q_all, pieces[0], preferred_element_type=jnp.float32)
    kv_full = jnp.dot(kv_all, pieces[1], preferred_element_type=jnp.float32)
    all_cos, all_sin = turn_tables(0, length)
    query_heads = make_queries(q_full, all_cos, all_sin, heads_here)
    keyval_heads = kv_full.astype(jnp.bfloat16)
    attended = attend(query_heads, keyval_heads, rot_all, heads_here)
    merged = lax.all_to_all(attended, "sp", split_axis=0, concat_axis=1, tiled=True)
    proj = jnp.dot(
        merged, lax.all_gather(w_out, "dp", axis=1, tiled=True), preferred_element_type=jnp.float32
    )
    mixed = norm_rows(proj, out_gain).astype(jnp.bfloat16)
    return mixed[None]


def turn_table(length):
    positions = np.arange(length, dtype=np.float32)
    freqs = np.float32(THETA) ** (-np.arange(0, ROPE, 2).astype(np.float32) / np.float32(ROPE))
    angles = positions[:, None] * freqs[None, :].astype(np.float32)
    cosine, sine = np.cos(angles), np.sin(angles)
    return np.concatenate([cosine, cosine, sine, sine], axis=1).astype(np.float32)


class Copies:
    def __init__(self, send_sems, recv_sems):
        self.send_sems, self.recv_sems = send_sems, recv_sems
        self.sends = self.receives = 0
        self.owed = []

    def reserve(self, count=1):
        at = self.receives
        self.receives += count
        assert self.receives <= self.recv_sems.shape[0]
        return at

    def reserve_send(self, whole, when=None):
        at = self.sends
        self.sends += 1
        assert self.sends <= self.send_sems.shape[0]
        self.owed.append((whole, at, when))
        return at

    def start(self, source, target, device, send_at, recv_at, when=None):
        def make():
            return pltpu.make_async_remote_copy(
                src_ref=source(),
                dst_ref=target(),
                send_sem=self.send_sems.at[send_at],
                recv_sem=self.recv_sems.at[recv_at],
                device_id=device,
                device_id_type=MESH,
            )

        guarded(when, lambda: make().start())

    def wait(self, whole, at):
        pltpu.make_async_copy(whole(), whole(), self.recv_sems.at[at]).wait()

    def drain(self):
        for whole, at, when in self.owed:
            guarded(
                when,
                lambda: pltpu.make_async_copy(whole(), whole(), self.send_sems.at[at]).wait(),
            )


def guarded(when, action):
    if when is None:
        action()
    else:

        @pl.when(when)
        def _():
            action()


class Direct:
    def __init__(self, copies, place, own, view, whole):
        self.copies, self.place, self.own, self.view = copies, place, own, view
        self.arrived = copies.reserve(place["z_count"])
        self.sent = copies.reserve_send(whole)

    def start(self):
        place = self.place
        for step in reversed(place["steps"]):
            self.copies.start(
                self.own,
                functools.partial(self.view, place["dp"]),
                {"dp": place["slots"][step]},
                self.sent,
                self.arrived + place["z"],
            )

    def forward(self, step):
        pass

    def settle(self, step):
        source, slot = self.place["order"][step], self.place["slots"][step]
        self.copies.wait(functools.partial(self.view, slot), self.arrived + source)


class Chain:
    def __init__(self, copies, place, own, view):
        self.copies, self.place, self.own, self.view = copies, place, own, view
        self.arrived = copies.reserve(place["z_count"])

    def start(self):
        place = self.place
        block = functools.partial(self.view, place["dp"])
        for way in (1, -1):
            onward = place["z"] + way
            when = place["above"] if way > 0 else place["below"]
            self.copies.start(
                self.own,
                block,
                {"dp": 2 * onward + place["side"]},
                self.copies.reserve_send(block, when),
                self.arrived + place["z"],
                when,
            )

    def passes(self, step):
        place, source = self.place, self.place["order"][step]
        rising = (source < place["z"]) & place["above"]
        sinking = (source > place["z"]) & place["below"]
        return rising, sinking

    def block(self, step):
        return functools.partial(self.view, self.place["slots"][step])

    def forward(self, step):
        place = self.place
        source, block = place["order"][step], self.block(step)
        rising, sinking = self.passes(step)
        sent = self.copies.reserve_send(block, rising | sinking)

        def move():
            self.copies.wait(block, self.arrived + source)
            for way in (1, -1):
                onward = place["z"] + way
                self.copies.start(
                    block,
                    block,
                    {"dp": 2 * onward + place["side"]},
                    sent,
                    self.arrived + source,
                    rising if way > 0 else sinking,
                )

        guarded(rising | sinking, move)

    def settle(self, step):
        source, block = self.place["order"][step], self.block(step)
        rising, sinking = self.passes(step)
        guarded(
            jnp.logical_not(rising | sinking),
            lambda: self.copies.wait(block, self.arrived + source),
        )


class PlaneSpread:
    def __init__(self, copies, place, view, span, rows, halves, sent):
        self.copies, self.place, self.view, self.rows = copies, place, view, rows
        self.span, self.halves, self.sent = span, halves, sent
        self.early_x, self.early_y, self.rest = (copies.reserve() for _ in range(3))

    def start(self, owner, begin, count, towards, recv_at):
        block = functools.partial(self.view, self.place[owner], begin, count)
        self.copies.start(block, block, {"sp": self.place[towards]}, self.sent, recv_at)

    def send(self):
        rows, half = self.rows, self.rows // 2
        if self.halves:
            self.start("me", 0, half, "x", self.early_x)
            self.start("me", half, half, "y", self.early_y)
            self.start("me", half, half, "x", self.rest)
            self.start("me", 0, half, "y", self.rest)
        else:
            self.start("me", 0, rows, "x", self.early_x)
            self.start("me", 0, rows, "y", self.early_y)

    def relay(self):
        half = self.rows // 2
        early = half if self.halves else self.rows
        self.copies.wait(functools.partial(self.view, self.place["x"], 0, early), self.early_x)
        self.start("x", 0, half, "y", self.rest)
        begin = half if self.halves else 0
        self.copies.wait(functools.partial(self.view, self.place["y"], begin, early), self.early_y)
        self.start("y", half, half, "x", self.rest)

    def finish(self):
        self.copies.wait(functools.partial(self.span, 4 if self.halves else 2), self.rest)


class Gather:
    def __init__(self, copies, place, buffer, groups):
        self.copies, self.place, self.buffer = copies, place, buffer
        self.crossed = [copies.reserve() for _ in range(groups)]
        self.cross_sent = copies.reserve_send(lambda: buffer.at[pl.ds(0, place["z_count"])])

    def cross(self, step, source, target):
        self.copies.start(
            source,
            target,
            {"dp": self.place["core"]},
            self.cross_sent,
            self.crossed[step % len(self.crossed)],
        )

    def keep(self):
        self.cross(0, self.own_whole, lambda: self.buffer.at[self.place["dp"]])

    def finish(self):
        self.copies.wait(lambda: self.buffer.at[pl.ds(0, self.place["z_count"])], self.crossed[0])

    def finish_step(self, step):
        self.copies.wait(lambda: self.buffer.at[0], self.crossed[step])


class WeightGather(Gather):
    def __init__(self, copies, place, source, buffer, tail=0, chunks=1, chained=False):
        super().__init__(copies, place, buffer, place["z_count"] if chained else 1)
        self.own_whole = (lambda: source) if chained else (lambda: buffer.at[place["dp"]])
        self.rows = (source.shape[0] - tail) // place["sp_count"]
        self.halves = chained
        self.planes = {}
        self.plane_sent = copies.reserve_send(
            lambda: buffer.at[pl.ds(0, len(place["steps"])), pl.ds(0, 3 * self.rows), :]
        )
        start = pl.multiple_of(place["me"] * self.rows, SUBLANES)
        own = lambda: source.at[pl.ds(start, self.rows), :]
        view = lambda slot: self.piece(slot, place["me"], 0, self.rows)
        if chained:
            self.chain = Chain(copies, place, own, view)
        else:
            whole = lambda: source.at[pl.ds(0, self.rows * len(place["steps"])), :]
            self.chain = Direct(copies, place, lambda: view(place["dp"]), view, whole)
        if tail:
            part = tail // chunks
            self.tails = []
            for at in range(source.shape[0] - tail, source.shape[0], part):
                rest = pl.ds(at, part)
                view = lambda slot, rest=rest: buffer.at[slot, rest, :]
                own = lambda rest=rest: source.at[rest, :]
                self.tails.append(Chain(copies, place, own, view))

    def piece(self, slot, owner, begin, count):
        start = pl.multiple_of(owner * self.rows + begin, SUBLANES)
        return self.buffer.at[slot, pl.ds(start, count), :]

    def span(self, halves):
        return self.buffer.at[0, pl.ds(0, halves * (self.rows // 2)), :]

    def cross_piece(self, step, owner):
        slot = self.place["slots"][step]
        block = lambda: self.piece(slot, self.place[owner], 0, self.rows)
        self.cross(step, block, block)

    def spread(self, step):
        self.chain.settle(step)
        view = functools.partial(self.piece, self.place["slots"][step])
        plane = PlaneSpread(
            self.copies, self.place, view, self.span, self.rows, self.halves, self.plane_sent
        )
        plane.send()
        self.planes[step] = plane
        self.cross_piece(step, "me")

    def relay(self, step):
        self.planes[step].relay()
        if not self.halves:
            self.cross_piece(step, "x")
            self.cross_piece(step, "y")

    def close(self, step):
        self.planes[step].finish()
        if self.halves:
            self.cross_piece(step, "x")
            self.cross_piece(step, "y")
        self.cross_piece(step, "far")

    def start_tail(self, chunk):
        self.tails[chunk].start()

    def forward_tail(self, chunk, step):
        self.tails[chunk].forward(step)

    def settle_tail(self, chunk, step):
        tail = self.tails[chunk]
        tail.settle(step)
        self.cross(step, tail.block(step), tail.block(step))


class ColumnGather(Gather):
    def __init__(self, copies, place, source, buffer):
        super().__init__(copies, place, buffer, 1)
        width = buffer.shape[2]
        start = pl.multiple_of(place["me"] * width, LANES)
        self.own_whole = lambda: source.at[:, pl.ds(start, width)]
        self.view = lambda slot: buffer.at[slot]
        self.chain = Chain(copies, place, self.own_whole, self.view)

    def settle(self, step):
        self.chain.settle(step)
        slot = self.place["slots"][step]
        block = lambda: self.view(slot)
        self.cross(step, block, block)


def nearest_first(z, z_count, step):
    short = jnp.minimum(z, z_count - 1 - z)
    long_way = jnp.where(2 * z < z_count - 1, 1, -1)
    turn = (step + 1) // 2
    both = z - long_way * turn if step % 2 else z + long_way * turn
    return jnp.where(step <= 2 * short, both, z + long_way * (step - short))


def rotary_picks(rows, offset, skip):
    width = skip + 2 * ROPE
    row = lax.broadcasted_iota(jnp.int32, (rows, width), 0)
    col = lax.broadcasted_iota(jnp.int32, (rows, width), 1)
    half = ROPE // 2
    minus = (col >= skip + ROPE) & (col < skip + ROPE + half)
    origin = jnp.where(
        col < skip + ROPE, col, jnp.where(minus, col - half, col - ROPE - half)
    )
    sign = jnp.where(minus, -1.0, 1.0)
    return jnp.where(row == origin + offset, sign, 0.0).astype(jnp.bfloat16)


def turned(values, table):
    product = values * table
    return product + pltpu.roll(product, ROPE, axis=1)


def dot(left, right):
    return jnp.dot(left, right, preferred_element_type=jnp.float32)


def kernel(
    sp_count, dp_count,
    tokens_in, w_qdown, w_kvdown, rotary_in, q_gain_in, kv_gain_in, w_qup, w_kvup, w_out,
    out_gain_in, table_in,
    out,
    tokens, w_rotary, q_gain, kv_gain, out_gain, table,
    qd_all, kvd_all, qu_all, kvu_all, wo_all, q_lat, kv_lat, rot_all,
    q_heads, k_heads, v_heads, qu_laid, attended, merged, proj,
    send_sems, recv_sems, back_send, back_recv, local_sems,
):
    scope = jax.named_scope
    me = lax.axis_index("sp")
    dp = lax.axis_index("dp")
    z_count = dp_count // 2
    side = lax.rem(dp, 2)
    z = dp // 2
    steps = range(1, z_count)
    order = {step: nearest_first(z, z_count, step) for step in steps}
    place = {
        "me": me,
        "dp": dp,
        "z": z,
        "side": side,
        "above": z < z_count - 1,
        "below": z > 0,
        "order": order,
        "slots": {step: 2 * order[step] + side for step in steps},
        "sp_count": sp_count,
        "dp_count": dp_count,
        "z_count": z_count,
        "steps": steps,
        "x": me + 1 - 2 * lax.rem(me, 2),
        "y": lax.rem(me + 2, sp_count),
        "far": sp_count - 1 - me,
        "core": dp + 1 - 2 * side,
    }
    count = tokens.shape[0]
    heads = q_heads.shape[0]
    rank = kvd_all.shape[2]

    barrier = pltpu.get_barrier_semaphore()

    def greet(peer):
        pl.semaphore_signal(barrier, inc=1, device_id=peer, device_id_type=MESH)

    for step in range(1, sp_count):
        greet({"sp": lax.rem(me + step, sp_count)})
    greet({"dp": place["core"]})
    for step in steps:
        greet({"dp": lax.rem(dp + 2 * step, dp_count)})

    copies = Copies(send_sems, recv_sems)
    kvd = WeightGather(copies, place, w_kvdown, kvd_all)
    qd = WeightGather(copies, place, w_qdown, qd_all)
    kvu = ColumnGather(copies, place, w_kvup, kvu_all)
    qu = ColumnGather(copies, place, w_qup, qu_all)
    wo = WeightGather(copies, place, w_out, wo_all, w_out.shape[0] * 7 // 16, chunks=CHUNKS, chained=True)
    places = [
        (w_kvdown, kvd_all.at[dp]),
        (rotary_in, w_rotary),
        (tokens_in, tokens),
        (table_in, table),
        (w_qdown, qd_all.at[dp]),
        (kv_gain_in, kv_gain),
        (q_gain_in, q_gain),
        (out_gain_in, out_gain),
        (qu.own_whole(), qu_all.at[dp]),
        (kvu.own_whole(), kvu_all.at[dp]),
        (w_out, wo_all.at[dp]),
    ]
    loads = [
        pltpu.make_async_copy(source, target, local_sems.at[at])
        for at, (source, target) in enumerate(places)
    ]
    for load in loads:
        load.start()

    with scope("barrier"):
        pl.semaphore_wait(barrier, sp_count + len(steps))

    loads[0].wait()
    kvd.chain.start()
    kvd.keep()
    for load in loads[1:8]:
        load.wait()
    for gather in (qd, kvu, qu, wo):
        gather.keep()

    with scope("keyrot"):
        own_table = table[pl.ds(pl.multiple_of(me * count, SUBLANES), count), :]
        picks = rotary_picks(ROPE, 0, 0)
        rotary = lax.dot_general(
            picks, w_rotary[...], (((0,), (0,)), ((), ())), preferred_element_type=jnp.float32
        ).astype(jnp.bfloat16)
        key_rot = lax.dot_general(
            tokens[...], rotary, (((1,), (1,)), ((), ())), preferred_element_type=jnp.float32
        )
        key_rot = turned(key_rot, own_table)
        lane = lax.broadcasted_iota(jnp.int32, key_rot.shape, 1)
        rot_all[me] = jnp.where(lane < ROPE, key_rot, 0.0).astype(jnp.bfloat16)

    last = steps[-1]

    def block_view(buffer, owner, begin, rows):
        return buffer.at[owner, pl.ds(begin, rows), :]

    def latent_plane(buffer):
        sent = copies.reserve_send(lambda: buffer.at[pl.ds(0, 3)])
        span = lambda halves: buffer.at[pl.ds(0, halves // 2)]
        view = functools.partial(block_view, buffer)
        return PlaneSpread(copies, place, view, span, count, True, sent)

    rot_plane = latent_plane(rot_all)
    kv_plane = latent_plane(kv_lat)
    q_plane = latent_plane(q_lat)

    def make_kv_latent():
        down = kvd_all[...].reshape(-1, rank)
        kv_lat[me] = norm_rows(dot(tokens[...], down), kv_gain[...]).astype(jnp.bfloat16)

    def make_q_latent():
        down = qd_all[...].reshape(-1, qd_all.shape[2])
        q_lat[me] = norm_rows(dot(tokens[...], down), q_gain[...]).astype(jnp.bfloat16)

    def lay_queries():
        laid = qu_all[...].reshape(-1, qu_all.shape[2])
        for head in range(heads):
            picks = rotary_picks(laid.shape[1], head * (NOPE + ROPE), NOPE)
            qu_laid[:, head * head_width : (head + 1) * head_width] = dot(laid, picks).astype(
                jnp.bfloat16
            )

    head_width = NOPE + 2 * ROPE

    def do(name, action, *args):
        with scope(name + "".join(str(a) for a in args)):
            action(*args)

    def make_keys(block, _):
        rows = pl.ds(pl.multiple_of(block * count, SUBLANES), count)
        latent = kv_lat[block]
        full = dot(latent, kvu_all[...].reshape(rank, -1)).astype(jnp.bfloat16)
        for head in range(heads):
            at = head * (NOPE + VDIM)
            k_heads[head, rows, :NOPE] = full[:, at : at + NOPE]
            k_heads[head, rows, NOPE:] = rot_all[block]
            v_heads[head, rows, :] = full[:, at + NOPE : at + NOPE + VDIM]
        return 0

    def make_all_keys():
        lax.fori_loop(0, sp_count, make_keys, 0)

    def make_block(block, _):
        rows = pl.ds(pl.multiple_of(block * count, SUBLANES), count)
        full = dot(q_lat[block], qu_laid[...])
        turns = table[rows, :]
        for head in range(heads):
            at = head * head_width
            q_heads[head, rows, :NOPE] = full[:, at : at + NOPE].astype(jnp.bfloat16)
            part = full[:, at + NOPE : at + head_width]
            q_heads[head, rows, NOPE:] = turned(part, turns).astype(jnp.bfloat16)
        return 0

    def make_all_queries():
        lax.fori_loop(0, sp_count, make_block, 0)

    factor = (NOPE + ROPE) ** (-0.5) * math.log2(math.e)
    contract = (((1,), (1,)), ((), ()))
    width = heads * VDIM

    def head_lanes(owner, head):
        return pl.ds(pl.multiple_of(owner * width + head * VDIM, LANES), VDIM)

    def back(block, head, source):
        return pltpu.make_async_remote_copy(
            src_ref=attended.at[block, :, head_lanes(0, head)],
            dst_ref=merged.at[:, head_lanes(source, head)],
            send_sem=back_send,
            recv_sem=back_recv,
            device_id={"sp": block},
            device_id_type=MESH,
        )

    def one_head(head, _):
        for block in reversed(range(sp_count)):
            begin = block * count
            query = q_heads[head, begin : begin + count, :]
            near = lax.dot_general(
                query, k_heads[head, begin : begin + count, :], contract,
                preferred_element_type=jnp.float32,
            )
            row = lax.broadcasted_iota(jnp.int32, near.shape, 0)
            col = lax.broadcasted_iota(jnp.int32, near.shape, 1)
            near = jnp.where(col <= row, near, -jnp.inf)
            top = jnp.max(near, axis=-1, keepdims=True)
            if block:
                far = lax.dot_general(
                    query, k_heads[head, :begin, :], contract, preferred_element_type=jnp.float32
                )
                top = jnp.maximum(top, jnp.max(far, axis=-1, keepdims=True))
            near = jnp.exp2((near - top) * factor)
            total = jnp.sum(near, axis=-1, keepdims=True)
            if block:
                far = jnp.exp2((far - top) * factor)
                total = total + jnp.sum(far, axis=-1, keepdims=True)
            share = 1.0 / total
            result = dot((near * share).astype(jnp.bfloat16), v_heads[head, begin : begin + count, :])
            if block:
                result = result + dot((far * share).astype(jnp.bfloat16), v_heads[head, :begin, :])
            attended[block, :, head_lanes(0, head)] = result.astype(jnp.bfloat16)
        for block in range(sp_count):

            @pl.when(me != block)
            def _():
                back(block, head, me).start()

        merged[:, head_lanes(me, head)] = attended[me, :, head_lanes(0, head)]
        return 0

    def attend_head(head):
        lax.fori_loop(head, head + 1, one_head, 0)

    others = attended.at[pl.ds(0, sp_count - 1)]
    out_width = wo_all.shape[2]

    def wait_back():
        pltpu.make_async_copy(others, others, back_recv).wait()

    def project(step, squares):
        with scope(f"project{step}"):
            for core in range(2):
                piece = 2 * (order[step] if step else z) + core
                lanes = pl.ds(pl.multiple_of(piece * out_width, LANES), out_width)
                value = dot(merged[...], wo_all[piece])
                proj[:, lanes] = value
                squares = squares + jnp.sum(value * value, axis=-1, keepdims=True)
        return squares

    rot_plane.send()
    do("kd_s", kvd.spread, 1)
    do("kd_s", kvd.spread, 2)
    qd.chain.start()
    do("rot_r", rot_plane.relay)
    do("kd_r", kvd.relay, 1)
    do("kd_s", kvd.spread, 3)
    kvu.chain.start()
    qu.chain.start()
    wo.chain.start()
    do("kd_r", kvd.relay, 2)
    do("kd_r", kvd.relay, 3)
    do("qd_s", qd.spread, 1)
    do("kd_c", kvd.close, 1)
    do("qd_s", qd.spread, 2)
    do("qd_s", qd.spread, 3)
    do("kd_c", kvd.close, 2)
    do("kd_c", kvd.close, 3)
    do("qd_r", qd.relay, 1)
    do("kvu_fw", kvu.chain.forward, 1)
    do("qu_fw", qu.chain.forward, 1)
    do("kvu_fw", kvu.chain.forward, 2)
    do("qu_fw", qu.chain.forward, 2)
    wo.start_tail(0)
    do("qd_r", qd.relay, 2)
    do("kd_f", kvd.finish)
    do("kv_lat", make_kv_latent)
    do("qd_r", qd.relay, 3)
    kv_plane.send()
    do("kvu_fw", kvu.chain.forward, 3)
    do("qu_fw", qu.chain.forward, 3)
    do("qd_c", qd.close, 1)
    do("qd_c", qd.close, 2)
    do("kv_r", kv_plane.relay)
    do("qd_c", qd.close, 3)
    do("qd_f", qd.finish)
    do("q_lat", make_q_latent)
    q_plane.send()
    do("wo_fw", wo.chain.forward, 1)
    do("wo_fw", wo.chain.forward, 2)
    do("q_r", q_plane.relay)
    do("wo_s", wo.spread, 1)
    do("wo_fw", wo.chain.forward, 3)
    do("t0_fw", wo.forward_tail, 0, 1)
    do("t0_fw", wo.forward_tail, 0, 2)
    wo.start_tail(1)
    do("qu_st", qu.settle, 1)
    do("kvu_st", kvu.settle, 1)
    do("qu_st", qu.settle, 2)
    do("kvu_st", kvu.settle, 2)
    do("qu_st", qu.settle, 3)
    do("kvu_st", kvu.settle, 3)
    loads[9].wait()
    do("kvu_f", kvu.finish)
    do("rot_f", rot_plane.finish)
    do("kv_f", kv_plane.finish)
    do("make_keys", make_all_keys)
    loads[8].wait()
    do("qu_f", qu.finish)
    do("qu_lay", lay_queries)
    do("wo_s", wo.spread, 2)
    do("wo_r", wo.relay, 1)
    do("q_f", q_plane.finish)
    do("make_q", make_all_queries)
    do("t0_fw", wo.forward_tail, 0, 3)
    do("attn", attend_head, 0)
    do("wo_s", wo.spread, 3)
    do("t1_fw", wo.forward_tail, 1, 1)
    do("t1_fw", wo.forward_tail, 1, 2)
    do("attn", attend_head, 1)
    do("wo_r", wo.relay, 2)
    do("attn", attend_head, 2)
    do("t1_fw", wo.forward_tail, 1, 3)
    do("wo_r", wo.relay, 3)
    do("attn", attend_head, 3)
    do("wo_c", wo.close, 1)
    do("t0_st", wo.settle_tail, 0, 1)
    do("t0_st", wo.settle_tail, 0, 2)
    do("t0_st", wo.settle_tail, 0, 3)
    do("t1_st", wo.settle_tail, 1, 1)
    do("wo_c", wo.close, 2)
    do("t1_st", wo.settle_tail, 1, 2)
    do("a2a", wait_back)
    squares = jnp.zeros((count, 1), jnp.float32)
    loads[10].wait()
    do("wo_f", wo.finish_step, 0)
    squares = project(0, squares)
    do("wo_f", wo.finish_step, 1)
    squares = project(1, squares)
    do("wo_c", wo.close, 3)
    do("t1_st", wo.settle_tail, 1, 3)
    do("wo_f", wo.finish_step, 2)
    squares = project(2, squares)
    do("wo_f", wo.finish_step, 3)
    squares = project(3, squares)
    with scope("norm"):
        scale = lax.rsqrt(squares * (1.0 / out.shape[1]) + EPSILON)
        out[...] = (proj[...] * scale * out_gain[...]).astype(out.dtype)
    with scope("drain"):
        copies.drain()
        pltpu.make_async_copy(others, others, back_send).wait()


def kernel_body(mesh, tokens, w_qdown, w_kvdown, w_rotary, q_gain, kv_gain, w_qup, w_kvup, w_out, out_gain):
    sp_count, dp_count = mesh.shape["sp"], mesh.shape["dp"]
    heads = HEADS // sp_count
    count, depth = tokens.shape[1:]
    length = count * sp_count
    q_rank, kv_rank = w_qdown.shape[1], w_kvdown.shape[1]
    bf16 = jnp.bfloat16
    steps = dp_count // 2 - 1
    chains = 3 + CHUNKS
    sends = chains * (steps + 2) + 13
    receives = 3 * 3 * steps + 9 + (chains + 2) * (steps + 1) + 4 + steps + 1
    vmem, hbm = pl.BlockSpec(memory_space=pltpu.VMEM), pl.BlockSpec(memory_space=pl.ANY)
    sp_width = HEADS // sp_count
    mixed = pl.pallas_call(
        functools.partial(kernel, sp_count, dp_count),
        out_shape=pltpu.VMEM((count, w_out.shape[1] * dp_count), bf16),
        in_specs=[hbm] * 11,
        out_specs=vmem,
        scratch_shapes=[
            pltpu.VMEM((count, depth), bf16),
            pltpu.VMEM(w_rotary.shape[::-1], bf16),
            pltpu.VMEM((1, q_rank), jnp.float32),
            pltpu.VMEM((1, kv_rank), jnp.float32),
            pltpu.VMEM((1, out_gain.shape[0]), jnp.float32),
            pltpu.VMEM((length, 4 * (ROPE // 2)), jnp.float32),
            pltpu.VMEM((dp_count,) + w_qdown.shape, bf16),
            pltpu.VMEM((dp_count,) + w_kvdown.shape, bf16),
            pltpu.VMEM((dp_count, w_qup.shape[0], sp_width * (NOPE + ROPE)), bf16),
            pltpu.VMEM((dp_count, w_kvup.shape[0], sp_width * (NOPE + VDIM)), bf16),
            pltpu.VMEM((dp_count,) + w_out.shape, bf16),
            pltpu.VMEM((sp_count, count, q_rank), bf16),
            pltpu.VMEM((sp_count, count, kv_rank), bf16),
            pltpu.VMEM((sp_count, count, 2 * ROPE), bf16),
            pltpu.VMEM((heads, length, NOPE + 2 * ROPE), bf16),
            pltpu.VMEM((heads, length, NOPE + 2 * ROPE), bf16),
            pltpu.VMEM((heads, length, VDIM), bf16),
            pltpu.VMEM((q_rank, heads * (NOPE + 2 * ROPE)), bf16),
            pltpu.VMEM((sp_count, count, heads * VDIM), bf16),
            pltpu.VMEM((count, HEADS * VDIM), bf16),
            pltpu.VMEM((count, w_out.shape[1] * dp_count), jnp.float32),
            pltpu.SemaphoreType.DMA((sends,)),
            pltpu.SemaphoreType.DMA((receives,)),
            pltpu.SemaphoreType.DMA,
            pltpu.SemaphoreType.DMA,
            pltpu.SemaphoreType.DMA((11,)),
        ],
        compiler_params=pltpu.CompilerParams(
            collective_id=0, has_side_effects=True, vmem_limit_bytes=60 * 1024 * 1024
        ),
        name="latent_attention",
    )(
        tokens[0], w_qdown, w_kvdown, w_rotary.T, q_gain[None], kv_gain[None], w_qup, w_kvup, w_out,
        out_gain[None], jnp.asarray(turn_table(length)),
    )
    return mixed[None]


def fits_kernel(mesh):
    return mesh.shape["sp"] == 2 * 2 and mesh.shape["dp"] % 2 == 0


def solution(mesh):
    in_specs = (
        P("dp", "sp", None),
        P("dp", None),
        P("dp", None),
        P(),
        P(),
        P(),
        P("dp", None),
        P("dp", None),
        P(None, "dp"),
        P(),
    )
    out_specs = P("dp", "sp", None)
    body = functools.partial(kernel_body, mesh) if fits_kernel(mesh) else plain_body
    return jax.shard_map(body, mesh=mesh, in_specs=in_specs, out_specs=out_specs, check_vma=False)
```

```python
import functools
import math

import jax
import jax.numpy as jnp
import numpy as np
from jax import lax
from jax.experimental import pallas as pl
from jax.experimental.pallas import tpu as pltpu
from jax.sharding import PartitionSpec as P

HEADS = 16
NOPE = 128
ROPE = 64
VDIM = 128


EPSILON = 1e-06
THETA = 10000.0
LANES = 128
SUBLANES = 16
CHUNKS = 2
MESH = pl.DeviceIdType.MESH


def norm_rows(values, gain):
    scale = lax.rsqrt(jnp.mean(values * values, axis=-1, keepdims=True) + EPSILON)
    return values * scale * gain


def rotate(values, cosine, sine):
    half = values.shape[-1] // 2
    first = values[..., :half]
    second = values[..., half:]
    return jnp.concatenate(
        [first * cosine - second * sine, second * cosine + first * sine], axis=-1
    )


def turn_tables(offset, count):
    positions = (offset + jnp.arange(count)).astype(jnp.float32)
    freqs = THETA ** (-jnp.arange(0, ROPE, 2).astype(jnp.float32) / ROPE)
    angles = positions[:, None] * freqs[None, :]
    return (jnp.cos(angles), jnp.sin(angles))


def make_queries(q_full, cosine, sine, heads_here):
    rows = q_full.shape[0]
    shaped = q_full.reshape(rows, heads_here, NOPE + ROPE)
    turned = rotate(shaped[..., NOPE:], cosine[:, None, :], sine[:, None, :])
    joined = jnp.concatenate([shaped[..., :NOPE], turned], axis=-1)
    return joined.reshape(rows, heads_here * (NOPE + ROPE)).astype(jnp.bfloat16)


def attend(query_heads, keyval_heads, key_rot, heads_here):
    length = query_heads.shape[0]
    block = math.gcd(length, 512)
    scaling = (NOPE + ROPE) ** (-0.5)
    queries = query_heads.reshape(length, heads_here, NOPE + ROPE)
    keyval = keyval_heads.reshape(length, heads_here, NOPE + VDIM)
    keys_all = keyval[..., :NOPE]
    values_all = keyval[..., NOPE:]
    outputs = []
    for begin in range(0, length, block):
        finish = begin + block
        query_block = queries[begin:finish]
        scores = jnp.einsum(
            "qhd,khd->hqk",
            query_block[..., :NOPE],
            keys_all[:finish],
            preferred_element_type=jnp.float32,
        )
        scores = scores + jnp.einsum(
            "qhd,kd->hqk",
            query_block[..., NOPE:],
            key_rot[:finish],
            preferred_element_type=jnp.float32,
        )
        scores = scores * scaling
        query_pos = begin + jnp.arange(block)
        key_pos = jnp.arange(finish)
        allowed = key_pos[None, :] <= query_pos[:, None]
        scores = jnp.where(allowed[None], scores, -jnp.inf)
        top = jnp.max(scores, axis=-1, keepdims=True)
        expo = jnp.exp(scores - top)
        weights = (expo / jnp.sum(expo, axis=-1, keepdims=True)).astype(jnp.bfloat16)
        attended = jnp.einsum(
            "hqk,khd->qhd", weights, values_all[:finish], preferred_element_type=jnp.float32
        )
        outputs.append(attended.astype(jnp.bfloat16))
    return jnp.concatenate(outputs, axis=0).reshape(length, heads_here * VDIM)


def plain_body(tokens, w_qdown, w_kvdown, w_rotary, q_gain, kv_gain, w_qup, w_kvup, w_out, out_gain):
    own_rows = tokens[0]
    tok_count = own_rows.shape[0]
    sp_count = lax.axis_size("sp")
    sp_place = lax.axis_index("sp")
    length = tok_count * sp_count
    heads_here = HEADS // sp_count
    pieces = (
        lax.all_gather(w_qdown, "dp", axis=0, tiled=True),
        lax.all_gather(w_kvdown, "dp", axis=0, tiled=True),
    )
    q_lat = jnp.dot(own_rows, pieces[0], preferred_element_type=jnp.float32)
    kv_lat = jnp.dot(own_rows, pieces[1], preferred_element_type=jnp.float32)
    q_norm = norm_rows(q_lat, q_gain).astype(jnp.bfloat16)
    kv_norm = norm_rows(kv_lat, kv_gain).astype(jnp.bfloat16)
    own_cos, own_sin = turn_tables(sp_place * tok_count, tok_count)
    key_rot = rotate(
        jnp.dot(own_rows, w_rotary, preferred_element_type=jnp.float32), own_cos, own_sin
    ).astype(jnp.bfloat16)
    q_all, kv_all, rot_all = (
        lax.all_gather(q_norm, "sp", axis=0, tiled=True),
        lax.all_gather(kv_norm, "sp", axis=0, tiled=True),
        lax.all_gather(key_rot, "sp", axis=0, tiled=True),
    )
    q_width = heads_here * (NOPE + ROPE)
    kv_width = heads_here * (NOPE + VDIM)
    q_columns = lax.dynamic_slice_in_dim(w_qup, sp_place * q_width, q_width, 1)
    kv_columns = lax.dynamic_slice_in_dim(w_kvup, sp_place * kv_width, kv_width, 1)
    pieces = (
        lax.all_gather(q_columns, "dp", axis=0, tiled=True),
        lax.all_gather(kv_columns, "dp", axis=0, tiled=True),
    )
    q_full = jnp.dot(q_all, pieces[0], preferred_element_type=jnp.float32)
    kv_full = jnp.dot(kv_all, pieces[1], preferred_element_type=jnp.float32)
    all_cos, all_sin = turn_tables(0, length)
    query_heads = make_queries(q_full, all_cos, all_sin, heads_here)
    keyval_heads = kv_full.astype(jnp.bfloat16)
    attended = attend(query_heads, keyval_heads, rot_all, heads_here)
    merged = lax.all_to_all(attended, "sp", split_axis=0, concat_axis=1, tiled=True)
    proj = jnp.dot(
        merged, lax.all_gather(w_out, "dp", axis=1, tiled=True), preferred_element_type=jnp.float32
    )
    mixed = norm_rows(proj, out_gain).astype(jnp.bfloat16)
    return mixed[None]


def turn_table(length):
    positions = np.arange(length, dtype=np.float32)
    freqs = np.float32(THETA) ** (-np.arange(0, ROPE, 2).astype(np.float32) / np.float32(ROPE))
    angles = positions[:, None] * freqs[None, :].astype(np.float32)
    cosine, sine = np.cos(angles), np.sin(angles)
    return np.concatenate([cosine, cosine, sine, sine], axis=1).astype(np.float32)


class Copies:
    def __init__(self, send_sems, recv_sems):
        self.send_sems, self.recv_sems = send_sems, recv_sems
        self.sends = self.receives = 0
        self.owed = []

    def reserve(self, count=1):
        at = self.receives
        self.receives += count
        assert self.receives <= self.recv_sems.shape[0]
        return at

    def reserve_send(self, whole, when=None):
        at = self.sends
        self.sends += 1
        assert self.sends <= self.send_sems.shape[0]
        self.owed.append((whole, at, when))
        return at

    def start(self, source, target, device, send_at, recv_at, when=None):
        def make():
            return pltpu.make_async_remote_copy(
                src_ref=source(),
                dst_ref=target(),
                send_sem=self.send_sems.at[send_at],
                recv_sem=self.recv_sems.at[recv_at],
                device_id=device,
                device_id_type=MESH,
            )

        guarded(when, lambda: make().start())

    def wait(self, whole, at):
        pltpu.make_async_copy(whole(), whole(), self.recv_sems.at[at]).wait()

    def drain(self):
        for whole, at, when in self.owed:
            guarded(
                when,
                lambda: pltpu.make_async_copy(whole(), whole(), self.send_sems.at[at]).wait(),
            )


def guarded(when, action):
    if when is None:
        action()
    else:

        @pl.when(when)
        def _():
            action()


class Direct:
    def __init__(self, copies, place, own, view, whole):
        self.copies, self.place, self.own, self.view = copies, place, own, view
        self.arrived = copies.reserve(place["z_count"])
        self.sent = copies.reserve_send(whole)

    def start(self):
        place = self.place
        for step in reversed(place["steps"]):
            self.copies.start(
                self.own,
                functools.partial(self.view, place["dp"]),
                {"dp": place["slots"][step]},
                self.sent,
                self.arrived + place["z"],
            )

    def forward(self, step):
        pass

    def settle(self, step):
        source, slot = self.place["order"][step], self.place["slots"][step]
        self.copies.wait(functools.partial(self.view, slot), self.arrived + source)


class Chain:
    def __init__(self, copies, place, own, view):
        self.copies, self.place, self.own, self.view = copies, place, own, view
        self.arrived = copies.reserve(place["z_count"])

    def start(self):
        place = self.place
        block = functools.partial(self.view, place["dp"])
        for way in (1, -1):
            onward = place["z"] + way
            when = place["above"] if way > 0 else place["below"]
            self.copies.start(
                self.own,
                block,
                {"dp": 2 * onward + place["side"]},
                self.copies.reserve_send(block, when),
                self.arrived + place["z"],
                when,
            )

    def passes(self, step):
        place, source = self.place, self.place["order"][step]
        rising = (source < place["z"]) & place["above"]
        sinking = (source > place["z"]) & place["below"]
        return rising, sinking

    def block(self, step):
        return functools.partial(self.view, self.place["slots"][step])

    def forward(self, step):
        place = self.place
        source, block = place["order"][step], self.block(step)
        rising, sinking = self.passes(step)
        sent = self.copies.reserve_send(block, rising | sinking)

        def move():
            self.copies.wait(block, self.arrived + source)
            for way in (1, -1):
                onward = place["z"] + way
                self.copies.start(
                    block,
                    block,
                    {"dp": 2 * onward + place["side"]},
                    sent,
                    self.arrived + source,
                    rising if way > 0 else sinking,
                )

        guarded(rising | sinking, move)

    def settle(self, step):
        source, block = self.place["order"][step], self.block(step)
        rising, sinking = self.passes(step)
        guarded(
            jnp.logical_not(rising | sinking),
            lambda: self.copies.wait(block, self.arrived + source),
        )


class PlaneSpread:
    def __init__(self, copies, place, view, span, rows, halves, sent):
        self.copies, self.place, self.view, self.rows = copies, place, view, rows
        self.span, self.halves, self.sent = span, halves, sent
        self.early_x, self.early_y, self.rest = (copies.reserve() for _ in range(3))

    def start(self, owner, begin, count, towards, recv_at):
        block = functools.partial(self.view, self.place[owner], begin, count)
        self.copies.start(block, block, {"sp": self.place[towards]}, self.sent, recv_at)

    def send(self):
        rows, half = self.rows, self.rows // 2
        if self.halves:
            self.start("me", 0, half, "x", self.early_x)
            self.start("me", half, half, "y", self.early_y)
            self.start("me", half, half, "x", self.rest)
            self.start("me", 0, half, "y", self.rest)
        else:
            self.start("me", 0, rows, "x", self.early_x)
            self.start("me", 0, rows, "y", self.early_y)

    def relay(self):
        half = self.rows // 2
        early = half if self.halves else self.rows
        self.copies.wait(functools.partial(self.view, self.place["x"], 0, early), self.early_x)
        self.start("x", 0, half, "y", self.rest)
        begin = half if self.halves else 0
        self.copies.wait(functools.partial(self.view, self.place["y"], begin, early), self.early_y)
        self.start("y", half, half, "x", self.rest)

    def finish(self):
        self.copies.wait(functools.partial(self.span, 4 if self.halves else 2), self.rest)


class Gather:
    def __init__(self, copies, place, buffer, groups):
        self.copies, self.place, self.buffer = copies, place, buffer
        self.crossed = [copies.reserve() for _ in range(groups)]
        self.cross_sent = copies.reserve_send(lambda: buffer.at[pl.ds(0, place["z_count"])])

    def cross(self, step, source, target):
        self.copies.start(
            source,
            target,
            {"dp": self.place["core"]},
            self.cross_sent,
            self.crossed[step % len(self.crossed)],
        )

    def keep(self):
        self.cross(0, self.own_whole, lambda: self.buffer.at[self.place["dp"]])

    def finish(self):
        self.copies.wait(lambda: self.buffer.at[pl.ds(0, self.place["z_count"])], self.crossed[0])

    def finish_step(self, step):
        self.copies.wait(lambda: self.buffer.at[0], self.crossed[step])


class WeightGather(Gather):
    def __init__(self, copies, place, source, buffer, tail=0, chunks=1, chained=False):
        super().__init__(copies, place, buffer, place["z_count"] if chained else 1)
        self.own_whole = (lambda: source) if chained else (lambda: buffer.at[place["dp"]])
        self.rows = (source.shape[0] - tail) // place["sp_count"]
        self.halves = chained
        self.planes = {}
        self.plane_sent = copies.reserve_send(
            lambda: buffer.at[pl.ds(0, len(place["steps"])), pl.ds(0, 3 * self.rows), :]
        )
        start = pl.multiple_of(place["me"] * self.rows, SUBLANES)
        own = lambda: source.at[pl.ds(start, self.rows), :]
        view = lambda slot: self.piece(slot, place["me"], 0, self.rows)
        if chained:
            self.chain = Chain(copies, place, own, view)
        else:
            whole = lambda: source.at[pl.ds(0, self.rows * len(place["steps"])), :]
            self.chain = Direct(copies, place, lambda: view(place["dp"]), view, whole)
        if tail:
            part = tail // chunks
            self.tails = []
            for at in range(source.shape[0] - tail, source.shape[0], part):
                rest = pl.ds(at, part)
                view = lambda slot, rest=rest: buffer.at[slot, rest, :]
                own = lambda rest=rest: source.at[rest, :]
                self.tails.append(Chain(copies, place, own, view))

    def piece(self, slot, owner, begin, count):
        start = pl.multiple_of(owner * self.rows + begin, SUBLANES)
        return self.buffer.at[slot, pl.ds(start, count), :]

    def span(self, halves):
        return self.buffer.at[0, pl.ds(0, halves * (self.rows // 2)), :]

    def cross_piece(self, step, owner):
        slot = self.place["slots"][step]
        block = lambda: self.piece(slot, self.place[owner], 0, self.rows)
        self.cross(step, block, block)

    def spread(self, step):
        self.chain.settle(step)
        view = functools.partial(self.piece, self.place["slots"][step])
        plane = PlaneSpread(
            self.copies, self.place, view, self.span, self.rows, self.halves, self.plane_sent
        )
        plane.send()
        self.planes[step] = plane
        self.cross_piece(step, "me")

    def relay(self, step):
        self.planes[step].relay()
        if not self.halves:
            self.cross_piece(step, "x")
            self.cross_piece(step, "y")

    def close(self, step):
        self.planes[step].finish()
        if self.halves:
            self.cross_piece(step, "x")
            self.cross_piece(step, "y")
        self.cross_piece(step, "far")

    def start_tail(self, chunk):
        self.tails[chunk].start()

    def forward_tail(self, chunk, step):
        self.tails[chunk].forward(step)

    def settle_tail(self, chunk, step):
        tail = self.tails[chunk]
        tail.settle(step)
        self.cross(step, tail.block(step), tail.block(step))


class ColumnGather(Gather):
    def __init__(self, copies, place, source, buffer):
        super().__init__(copies, place, buffer, 1)
        width = buffer.shape[2]
        start = pl.multiple_of(place["me"] * width, LANES)
        self.own_whole = lambda: source.at[:, pl.ds(start, width)]
        self.view = lambda slot: buffer.at[slot]
        self.chain = Chain(copies, place, self.own_whole, self.view)

    def settle(self, step):
        self.chain.settle(step)
        slot = self.place["slots"][step]
        block = lambda: self.view(slot)
        self.cross(step, block, block)


def nearest_first(z, z_count, step):
    short = jnp.minimum(z, z_count - 1 - z)
    long_way = jnp.where(2 * z < z_count - 1, 1, -1)
    turn = (step + 1) // 2
    both = z - long_way * turn if step % 2 else z + long_way * turn
    return jnp.where(step <= 2 * short, both, z + long_way * (step - short))


def rotary_picks(rows, offset, skip):
    width = skip + 2 * ROPE
    row = lax.broadcasted_iota(jnp.int32, (rows, width), 0)
    col = lax.broadcasted_iota(jnp.int32, (rows, width), 1)
    half = ROPE // 2
    minus = (col >= skip + ROPE) & (col < skip + ROPE + half)
    origin = jnp.where(
        col < skip + ROPE, col, jnp.where(minus, col - half, col - ROPE - half)
    )
    sign = jnp.where(minus, -1.0, 1.0)
    return jnp.where(row == origin + offset, sign, 0.0).astype(jnp.bfloat16)


def turned(values, table):
    product = values * table
    return product + pltpu.roll(product, ROPE, axis=1)


def dot(left, right):
    return jnp.dot(left, right, preferred_element_type=jnp.float32)


def kernel(
    sp_count, dp_count,
    tokens_in, w_qdown, w_kvdown, rotary_in, q_gain_in, kv_gain_in, w_qup, w_kvup, w_out,
    out_gain_in, table_in,
    out,
    tokens, w_rotary, q_gain, kv_gain, out_gain, table,
    qd_all, kvd_all, qu_all, kvu_all, wo_all, q_lat, kv_lat, rot_all,
    q_heads, k_heads, v_heads, qu_laid, attended, merged, proj,
    send_sems, recv_sems, back_send, back_recv, local_sems,
):
    scope = jax.named_scope
    me = lax.axis_index("sp")
    dp = lax.axis_index("dp")
    z_count = dp_count // 2
    side = lax.rem(dp, 2)
    z = dp // 2
    steps = range(1, z_count)
    order = {step: nearest_first(z, z_count, step) for step in steps}
    place = {
        "me": me,
        "dp": dp,
        "z": z,
        "side": side,
        "above": z < z_count - 1,
        "below": z > 0,
        "order": order,
        "slots": {step: 2 * order[step] + side for step in steps},
        "sp_count": sp_count,
        "dp_count": dp_count,
        "z_count": z_count,
        "steps": steps,
        "x": me + 1 - 2 * lax.rem(me, 2),
        "y": lax.rem(me + 2, sp_count),
        "far": sp_count - 1 - me,
        "core": dp + 1 - 2 * side,
    }
    count = tokens.shape[0]
    heads = q_heads.shape[0]
    rank = kvd_all.shape[2]

    barrier = pltpu.get_barrier_semaphore()

    def greet(peer):
        pl.semaphore_signal(barrier, inc=1, device_id=peer, device_id_type=MESH)

    for step in range(1, sp_count):
        greet({"sp": lax.rem(me + step, sp_count)})
    greet({"dp": place["core"]})
    for step in steps:
        greet({"dp": lax.rem(dp + 2 * step, dp_count)})

    copies = Copies(send_sems, recv_sems)
    kvd = WeightGather(copies, place, w_kvdown, kvd_all)
    qd = WeightGather(copies, place, w_qdown, qd_all)
    kvu = ColumnGather(copies, place, w_kvup, kvu_all)
    qu = ColumnGather(copies, place, w_qup, qu_all)
    wo = WeightGather(copies, place, w_out, wo_all, w_out.shape[0] * 7 // 16, chunks=CHUNKS, chained=True)
    places = [
        (w_kvdown, kvd_all.at[dp]),
        (rotary_in, w_rotary),
        (tokens_in, tokens),
        (table_in, table),
        (w_qdown, qd_all.at[dp]),
        (kv_gain_in, kv_gain),
        (q_gain_in, q_gain),
        (out_gain_in, out_gain),
        (qu.own_whole(), qu_all.at[dp]),
        (kvu.own_whole(), kvu_all.at[dp]),
        (w_out, wo_all.at[dp]),
    ]
    loads = [
        pltpu.make_async_copy(source, target, local_sems.at[at])
        for at, (source, target) in enumerate(places)
    ]
    for load in loads:
        load.start()

    with scope("barrier"):
        pl.semaphore_wait(barrier, sp_count + len(steps))

    loads[0].wait()
    kvd.chain.start()
    kvd.keep()
    for load in loads[1:8]:
        load.wait()
    for gather in (qd, kvu, qu, wo):
        gather.keep()

    with scope("keyrot"):
        own_table = table[pl.ds(pl.multiple_of(me * count, SUBLANES), count), :]
        picks = rotary_picks(ROPE, 0, 0)
        rotary = lax.dot_general(
            picks, w_rotary[...], (((0,), (0,)), ((), ())), preferred_element_type=jnp.float32
        ).astype(jnp.bfloat16)
        key_rot = lax.dot_general(
            tokens[...], rotary, (((1,), (1,)), ((), ())), preferred_element_type=jnp.float32
        )
        key_rot = turned(key_rot, own_table)
        lane = lax.broadcasted_iota(jnp.int32, key_rot.shape, 1)
        rot_all[me] = jnp.where(lane < ROPE, key_rot, 0.0).astype(jnp.bfloat16)

    last = steps[-1]

    def block_view(buffer, owner, begin, rows):
        return buffer.at[owner, pl.ds(begin, rows), :]

    def latent_plane(buffer):
        sent = copies.reserve_send(lambda: buffer.at[pl.ds(0, 3)])
        span = lambda halves: buffer.at[pl.ds(0, halves // 2)]
        view = functools.partial(block_view, buffer)
        return PlaneSpread(copies, place, view, span, count, True, sent)

    rot_plane = latent_plane(rot_all)
    kv_plane = latent_plane(kv_lat)
    q_plane = latent_plane(q_lat)

    def make_kv_latent():
        down = kvd_all[...].reshape(-1, rank)
        kv_lat[me] = norm_rows(dot(tokens[...], down), kv_gain[...]).astype(jnp.bfloat16)

    def make_q_latent():
        down = qd_all[...].reshape(-1, qd_all.shape[2])
        q_lat[me] = norm_rows(dot(tokens[...], down), q_gain[...]).astype(jnp.bfloat16)

    def lay_queries():
        laid = qu_all[...].reshape(-1, qu_all.shape[2])
        for head in range(heads):
            picks = rotary_picks(laid.shape[1], head * (NOPE + ROPE), NOPE)
            qu_laid[:, head * head_width : (head + 1) * head_width] = dot(laid, picks).astype(
                jnp.bfloat16
            )

    head_width = NOPE + 2 * ROPE

    def do(name, action, *args):
        with scope(name + "".join(str(a) for a in args)):
            action(*args)

    def make_keys(block, _):
        rows = pl.ds(pl.multiple_of(block * count, SUBLANES), count)
        latent = kv_lat[block]
        full = dot(latent, kvu_all[...].reshape(rank, -1)).astype(jnp.bfloat16)
        for head in range(heads):
            at = head * (NOPE + VDIM)
            k_heads[head, rows, :NOPE] = full[:, at : at + NOPE]
            k_heads[head, rows, NOPE:] = rot_all[block]
            v_heads[head, rows, :] = full[:, at + NOPE : at + NOPE + VDIM]
        return 0

    def make_all_keys():
        lax.fori_loop(0, sp_count, make_keys, 0)

    def make_block(block, _):
        rows = pl.ds(pl.multiple_of(block * count, SUBLANES), count)
        full = dot(q_lat[block], qu_laid[...])
        turns = table[rows, :]
        for head in range(heads):
            at = head * head_width
            q_heads[head, rows, :NOPE] = full[:, at : at + NOPE].astype(jnp.bfloat16)
            part = full[:, at + NOPE : at + head_width]
            q_heads[head, rows, NOPE:] = turned(part, turns).astype(jnp.bfloat16)
        return 0

    def make_all_queries():
        lax.fori_loop(0, sp_count, make_block, 0)

    factor = (NOPE + ROPE) ** (-0.5) * math.log2(math.e)
    contract = (((1,), (1,)), ((), ()))
    width = heads * VDIM

    def head_lanes(owner, head):
        return pl.ds(pl.multiple_of(owner * width + head * VDIM, LANES), VDIM)

    def merged_lanes(source, head):
        return pl.ds(pl.multiple_of(head * (sp_count * VDIM) + source * VDIM, LANES), VDIM)

    def back(block, head, source):
        return pltpu.make_async_remote_copy(
            src_ref=attended.at[block, :, head_lanes(0, head)],
            dst_ref=merged.at[:, merged_lanes(source, head)],
            send_sem=back_send,
            recv_sem=back_recv.at[head],
            device_id={"sp": block},
            device_id_type=MESH,
        )

    def one_head(head, _):
        for block in reversed(range(sp_count)):
            begin = block * count
            query = q_heads[head, begin : begin + count, :]
            near = lax.dot_general(
                query, k_heads[head, begin : begin + count, :], contract,
                preferred_element_type=jnp.float32,
            )
            row = lax.broadcasted_iota(jnp.int32, near.shape, 0)
            col = lax.broadcasted_iota(jnp.int32, near.shape, 1)
            near = jnp.where(col <= row, near, -jnp.inf)
            top = jnp.max(near, axis=-1, keepdims=True)
            if block:
                far = lax.dot_general(
                    query, k_heads[head, :begin, :], contract, preferred_element_type=jnp.float32
                )
                top = jnp.maximum(top, jnp.max(far, axis=-1, keepdims=True))
            near = jnp.exp2((near - top) * factor)
            total = jnp.sum(near, axis=-1, keepdims=True)
            if block:
                far = jnp.exp2((far - top) * factor)
                total = total + jnp.sum(far, axis=-1, keepdims=True)
            share = 1.0 / total
            result = dot((near * share).astype(jnp.bfloat16), v_heads[head, begin : begin + count, :])
            if block:
                result = result + dot((far * share).astype(jnp.bfloat16), v_heads[head, :begin, :])
            attended[block, :, head_lanes(0, head)] = result.astype(jnp.bfloat16)
        for block in range(sp_count):

            @pl.when(me != block)
            def _():
                back(block, head, me).start()

        merged[:, merged_lanes(me, head)] = attended[me, :, head_lanes(0, head)]
        return 0

    def attend_head(head):
        lax.fori_loop(head, head + 1, one_head, 0)

    others = attended.at[pl.ds(0, sp_count - 1)]
    out_width = wo_all.shape[2]

    def wait_back(begin, finish):
        for head in range(begin, finish):
            part = attended.at[pl.ds(0, sp_count - 1), :, head_lanes(0, head)]
            pltpu.make_async_copy(part, part, back_recv.at[head]).wait()

    def project(step, begin, finish):
        squares = jnp.zeros((count, 1), jnp.float32)
        for core in range(2):
            piece = 2 * (order[step] if step else z) + core
            lanes = pl.ds(pl.multiple_of(piece * out_width, LANES), out_width)
            rows = [
                wo_all[piece, pl.ds(source * width + head * VDIM, VDIM), :]
                for head in range(begin, finish)
                for source in range(sp_count)
            ]
            whole = sp_count * VDIM
            value = dot(merged[:, begin * whole : finish * whole], jnp.concatenate(rows, axis=0))
            if begin:
                value = value + proj[:, lanes]
            proj[:, lanes] = value
            if finish == heads:
                squares = squares + jnp.sum(value * value, axis=-1, keepdims=True)
        return squares

    rot_plane.send()
    do("kd_s", kvd.spread, 1)
    do("kd_s", kvd.spread, 2)
    qd.chain.start()
    do("rot_r", rot_plane.relay)
    do("kd_r", kvd.relay, 1)
    do("kd_s", kvd.spread, 3)
    kvu.chain.start()
    qu.chain.start()
    wo.chain.start()
    do("kd_r", kvd.relay, 2)
    do("kd_r", kvd.relay, 3)
    do("qd_s", qd.spread, 1)
    do("kd_c", kvd.close, 1)
    do("qd_s", qd.spread, 2)
    do("qd_s", qd.spread, 3)
    do("kd_c", kvd.close, 2)
    do("kd_c", kvd.close, 3)
    do("qd_r", qd.relay, 1)
    do("kvu_fw", kvu.chain.forward, 1)
    do("qu_fw", qu.chain.forward, 1)
    do("kvu_fw", kvu.chain.forward, 2)
    do("qu_fw", qu.chain.forward, 2)
    wo.start_tail(0)
    do("qd_r", qd.relay, 2)
    do("kd_f", kvd.finish)
    do("kv_lat", make_kv_latent)
    do("qd_r", qd.relay, 3)
    kv_plane.send()
    do("kvu_fw", kvu.chain.forward, 3)
    do("qu_fw", qu.chain.forward, 3)
    do("qd_c", qd.close, 1)
    do("qd_c", qd.close, 2)
    do("kv_r", kv_plane.relay)
    do("qd_c", qd.close, 3)
    do("qd_f", qd.finish)
    do("q_lat", make_q_latent)
    q_plane.send()
    do("wo_fw", wo.chain.forward, 1)
    do("wo_fw", wo.chain.forward, 2)
    do("q_r", q_plane.relay)
    do("wo_s", wo.spread, 1)
    do("wo_fw", wo.chain.forward, 3)
    do("t0_fw", wo.forward_tail, 0, 1)
    do("t0_fw", wo.forward_tail, 0, 2)
    wo.start_tail(1)
    do("qu_st", qu.settle, 1)
    do("kvu_st", kvu.settle, 1)
    do("qu_st", qu.settle, 2)
    do("kvu_st", kvu.settle, 2)
    do("qu_st", qu.settle, 3)
    do("kvu_st", kvu.settle, 3)
    loads[9].wait()
    do("kvu_f", kvu.finish)
    do("rot_f", rot_plane.finish)
    do("kv_f", kv_plane.finish)
    do("make_keys", make_all_keys)
    loads[8].wait()
    do("qu_f", qu.finish)
    do("qu_lay", lay_queries)
    do("wo_s", wo.spread, 2)
    do("wo_r", wo.relay, 1)
    do("q_f", q_plane.finish)
    do("make_q", make_all_queries)
    do("t0_fw", wo.forward_tail, 0, 3)
    do("attn", attend_head, 0)
    do("wo_s", wo.spread, 3)
    do("t1_fw", wo.forward_tail, 1, 1)
    do("t1_fw", wo.forward_tail, 1, 2)
    do("attn", attend_head, 1)
    do("wo_r", wo.relay, 2)
    do("attn", attend_head, 2)
    do("t1_fw", wo.forward_tail, 1, 3)
    do("wo_r", wo.relay, 3)
    do("attn", attend_head, 3)
    do("wo_c", wo.close, 1)
    do("t0_st", wo.settle_tail, 0, 1)
    do("t0_st", wo.settle_tail, 0, 2)
    do("t0_st", wo.settle_tail, 0, 3)
    do("t1_st", wo.settle_tail, 1, 1)
    do("wo_c", wo.close, 2)
    do("t1_st", wo.settle_tail, 1, 2)
    do("a2a", wait_back, 0, 3)
    squares = jnp.zeros((count, 1), jnp.float32)
    loads[10].wait()
    do("wo_f", wo.finish_step, 0)
    with scope("project00"):
        project(0, 0, 3)
    do("wo_f", wo.finish_step, 1)
    with scope("project10"):
        project(1, 0, 3)
    do("wo_f", wo.finish_step, 2)
    with scope("project20"):
        project(2, 0, 3)
    do("wo_c", wo.close, 3)
    do("a2a", wait_back, 3, 4)
    with scope("project03"):
        squares = squares + project(0, 3, 4)
    with scope("project13"):
        squares = squares + project(1, 3, 4)
    with scope("project23"):
        squares = squares + project(2, 3, 4)
    do("t1_st", wo.settle_tail, 1, 3)
    do("wo_f", wo.finish_step, 3)
    with scope("project30"):
        squares = squares + project(3, 0, 4)
    with scope("norm"):
        scale = lax.rsqrt(squares * (1.0 / out.shape[1]) + EPSILON)
        out[...] = (proj[...] * scale * out_gain[...]).astype(out.dtype)
    with scope("drain"):
        copies.drain()
        pltpu.make_async_copy(others, others, back_send).wait()


def kernel_body(mesh, tokens, w_qdown, w_kvdown, w_rotary, q_gain, kv_gain, w_qup, w_kvup, w_out, out_gain):
    sp_count, dp_count = mesh.shape["sp"], mesh.shape["dp"]
    heads = HEADS // sp_count
    count, depth = tokens.shape[1:]
    length = count * sp_count
    q_rank, kv_rank = w_qdown.shape[1], w_kvdown.shape[1]
    bf16 = jnp.bfloat16
    steps = dp_count // 2 - 1
    chains = 3 + CHUNKS
    sends = chains * (steps + 2) + 13
    receives = 3 * 3 * steps + 9 + (chains + 2) * (steps + 1) + 4 + steps + 1
    vmem, hbm = pl.BlockSpec(memory_space=pltpu.VMEM), pl.BlockSpec(memory_space=pl.ANY)
    sp_width = HEADS // sp_count
    mixed = pl.pallas_call(
        functools.partial(kernel, sp_count, dp_count),
        out_shape=pltpu.VMEM((count, w_out.shape[1] * dp_count), bf16),
        in_specs=[hbm] * 11,
        out_specs=vmem,
        scratch_shapes=[
            pltpu.VMEM((count, depth), bf16),
            pltpu.VMEM(w_rotary.shape[::-1], bf16),
            pltpu.VMEM((1, q_rank), jnp.float32),
            pltpu.VMEM((1, kv_rank), jnp.float32),
            pltpu.VMEM((1, out_gain.shape[0]), jnp.float32),
            pltpu.VMEM((length, 4 * (ROPE // 2)), jnp.float32),
            pltpu.VMEM((dp_count,) + w_qdown.shape, bf16),
            pltpu.VMEM((dp_count,) + w_kvdown.shape, bf16),
            pltpu.VMEM((dp_count, w_qup.shape[0], sp_width * (NOPE + ROPE)), bf16),
            pltpu.VMEM((dp_count, w_kvup.shape[0], sp_width * (NOPE + VDIM)), bf16),
            pltpu.VMEM((dp_count,) + w_out.shape, bf16),
            pltpu.VMEM((sp_count, count, q_rank), bf16),
            pltpu.VMEM((sp_count, count, kv_rank), bf16),
            pltpu.VMEM((sp_count, count, 2 * ROPE), bf16),
            pltpu.VMEM((heads, length, NOPE + 2 * ROPE), bf16),
            pltpu.VMEM((heads, length, NOPE + 2 * ROPE), bf16),
            pltpu.VMEM((heads, length, VDIM), bf16),
            pltpu.VMEM((q_rank, heads * (NOPE + 2 * ROPE)), bf16),
            pltpu.VMEM((sp_count, count, heads * VDIM), bf16),
            pltpu.VMEM((count, HEADS * VDIM), bf16),
            pltpu.VMEM((count, w_out.shape[1] * dp_count), jnp.float32),
            pltpu.SemaphoreType.DMA((sends,)),
            pltpu.SemaphoreType.DMA((receives,)),
            pltpu.SemaphoreType.DMA,
            pltpu.SemaphoreType.DMA((heads,)),
            pltpu.SemaphoreType.DMA((11,)),
        ],
        compiler_params=pltpu.CompilerParams(
            collective_id=0, has_side_effects=True, vmem_limit_bytes=60 * 1024 * 1024
        ),
        name="latent_attention",
    )(
        tokens[0], w_qdown, w_kvdown, w_rotary.T, q_gain[None], kv_gain[None], w_qup, w_kvup, w_out,
        out_gain[None], jnp.asarray(turn_table(length)),
    )
    return mixed[None]


def fits_kernel(mesh):
    return mesh.shape["sp"] == 2 * 2 and mesh.shape["dp"] % 2 == 0


def solution(mesh):
    in_specs = (
        P("dp", "sp", None),
        P("dp", None),
        P("dp", None),
        P(),
        P(),
        P(),
        P("dp", None),
        P("dp", None),
        P(None, "dp"),
        P(),
    )
    out_specs = P("dp", "sp", None)
    body = functools.partial(kernel_body, mesh) if fits_kernel(mesh) else plain_body
    return jax.shard_map(body, mesh=mesh, in_specs=in_specs, out_specs=out_specs, check_vma=False)
```

```python
import functools
import math

import jax
import jax.numpy as jnp
import numpy as np
from jax import lax
from jax.experimental import pallas as pl
from jax.experimental.pallas import tpu as pltpu
from jax.sharding import PartitionSpec as P

HEADS = 16
NOPE = 128
ROPE = 64
VDIM = 128


EPSILON = 1e-06
THETA = 10000.0
LANES = 128
SUBLANES = 16
CHUNKS = 2
MESH = pl.DeviceIdType.MESH


def norm_rows(values, gain):
    scale = lax.rsqrt(jnp.mean(values * values, axis=-1, keepdims=True) + EPSILON)
    return values * scale * gain


def rotate(values, cosine, sine):
    half = values.shape[-1] // 2
    first = values[..., :half]
    second = values[..., half:]
    return jnp.concatenate(
        [first * cosine - second * sine, second * cosine + first * sine], axis=-1
    )


def turn_tables(offset, count):
    positions = (offset + jnp.arange(count)).astype(jnp.float32)
    freqs = THETA ** (-jnp.arange(0, ROPE, 2).astype(jnp.float32) / ROPE)
    angles = positions[:, None] * freqs[None, :]
    return (jnp.cos(angles), jnp.sin(angles))


def make_queries(q_full, cosine, sine, heads_here):
    rows = q_full.shape[0]
    shaped = q_full.reshape(rows, heads_here, NOPE + ROPE)
    turned = rotate(shaped[..., NOPE:], cosine[:, None, :], sine[:, None, :])
    joined = jnp.concatenate([shaped[..., :NOPE], turned], axis=-1)
    return joined.reshape(rows, heads_here * (NOPE + ROPE)).astype(jnp.bfloat16)


def attend(query_heads, keyval_heads, key_rot, heads_here):
    length = query_heads.shape[0]
    block = math.gcd(length, 512)
    scaling = (NOPE + ROPE) ** (-0.5)
    queries = query_heads.reshape(length, heads_here, NOPE + ROPE)
    keyval = keyval_heads.reshape(length, heads_here, NOPE + VDIM)
    keys_all = keyval[..., :NOPE]
    values_all = keyval[..., NOPE:]
    outputs = []
    for begin in range(0, length, block):
        finish = begin + block
        query_block = queries[begin:finish]
        scores = jnp.einsum(
            "qhd,khd->hqk",
            query_block[..., :NOPE],
            keys_all[:finish],
            preferred_element_type=jnp.float32,
        )
        scores = scores + jnp.einsum(
            "qhd,kd->hqk",
            query_block[..., NOPE:],
            key_rot[:finish],
            preferred_element_type=jnp.float32,
        )
        scores = scores * scaling
        query_pos = begin + jnp.arange(block)
        key_pos = jnp.arange(finish)
        allowed = key_pos[None, :] <= query_pos[:, None]
        scores = jnp.where(allowed[None], scores, -jnp.inf)
        top = jnp.max(scores, axis=-1, keepdims=True)
        expo = jnp.exp(scores - top)
        weights = (expo / jnp.sum(expo, axis=-1, keepdims=True)).astype(jnp.bfloat16)
        attended = jnp.einsum(
            "hqk,khd->qhd", weights, values_all[:finish], preferred_element_type=jnp.float32
        )
        outputs.append(attended.astype(jnp.bfloat16))
    return jnp.concatenate(outputs, axis=0).reshape(length, heads_here * VDIM)


def plain_body(tokens, w_qdown, w_kvdown, w_rotary, q_gain, kv_gain, w_qup, w_kvup, w_out, out_gain):
    own_rows = tokens[0]
    tok_count = own_rows.shape[0]
    sp_count = lax.axis_size("sp")
    sp_place = lax.axis_index("sp")
    length = tok_count * sp_count
    heads_here = HEADS // sp_count
    pieces = (
        lax.all_gather(w_qdown, "dp", axis=0, tiled=True),
        lax.all_gather(w_kvdown, "dp", axis=0, tiled=True),
    )
    q_lat = jnp.dot(own_rows, pieces[0], preferred_element_type=jnp.float32)
    kv_lat = jnp.dot(own_rows, pieces[1], preferred_element_type=jnp.float32)
    q_norm = norm_rows(q_lat, q_gain).astype(jnp.bfloat16)
    kv_norm = norm_rows(kv_lat, kv_gain).astype(jnp.bfloat16)
    own_cos, own_sin = turn_tables(sp_place * tok_count, tok_count)
    key_rot = rotate(
        jnp.dot(own_rows, w_rotary, preferred_element_type=jnp.float32), own_cos, own_sin
    ).astype(jnp.bfloat16)
    q_all, kv_all, rot_all = (
        lax.all_gather(q_norm, "sp", axis=0, tiled=True),
        lax.all_gather(kv_norm, "sp", axis=0, tiled=True),
        lax.all_gather(key_rot, "sp", axis=0, tiled=True),
    )
    q_width = heads_here * (NOPE + ROPE)
    kv_width = heads_here * (NOPE + VDIM)
    q_columns = lax.dynamic_slice_in_dim(w_qup, sp_place * q_width, q_width, 1)
    kv_columns = lax.dynamic_slice_in_dim(w_kvup, sp_place * kv_width, kv_width, 1)
    pieces = (
        lax.all_gather(q_columns, "dp", axis=0, tiled=True),
        lax.all_gather(kv_columns, "dp", axis=0, tiled=True),
    )
    q_full = jnp.dot(q_all, pieces[0], preferred_element_type=jnp.float32)
    kv_full = jnp.dot(kv_all, pieces[1], preferred_element_type=jnp.float32)
    all_cos, all_sin = turn_tables(0, length)
    query_heads = make_queries(q_full, all_cos, all_sin, heads_here)
    keyval_heads = kv_full.astype(jnp.bfloat16)
    attended = attend(query_heads, keyval_heads, rot_all, heads_here)
    merged = lax.all_to_all(attended, "sp", split_axis=0, concat_axis=1, tiled=True)
    proj = jnp.dot(
        merged, lax.all_gather(w_out, "dp", axis=1, tiled=True), preferred_element_type=jnp.float32
    )
    mixed = norm_rows(proj, out_gain).astype(jnp.bfloat16)
    return mixed[None]


def turn_table(length):
    positions = np.arange(length, dtype=np.float32)
    freqs = np.float32(THETA) ** (-np.arange(0, ROPE, 2).astype(np.float32) / np.float32(ROPE))
    angles = positions[:, None] * freqs[None, :].astype(np.float32)
    cosine, sine = np.cos(angles), np.sin(angles)
    return np.concatenate([cosine, cosine, sine, sine], axis=1).astype(np.float32)


class Copies:
    def __init__(self, send_sems, recv_sems):
        self.send_sems, self.recv_sems = send_sems, recv_sems
        self.sends = self.receives = 0
        self.owed = []

    def reserve(self, count=1):
        at = self.receives
        self.receives += count
        assert self.receives <= self.recv_sems.shape[0]
        return at

    def reserve_send(self, whole, when=None):
        at = self.sends
        self.sends += 1
        assert self.sends <= self.send_sems.shape[0]
        self.owed.append((whole, at, when))
        return at

    def start(self, source, target, device, send_at, recv_at, when=None):
        def make():
            return pltpu.make_async_remote_copy(
                src_ref=source(),
                dst_ref=target(),
                send_sem=self.send_sems.at[send_at],
                recv_sem=self.recv_sems.at[recv_at],
                device_id=device,
                device_id_type=MESH,
            )

        guarded(when, lambda: make().start())

    def wait(self, whole, at):
        pltpu.make_async_copy(whole(), whole(), self.recv_sems.at[at]).wait()

    def drain(self):
        for whole, at, when in self.owed:
            guarded(
                when,
                lambda: pltpu.make_async_copy(whole(), whole(), self.send_sems.at[at]).wait(),
            )


def guarded(when, action):
    if when is None:
        action()
    else:

        @pl.when(when)
        def _():
            action()


class Direct:
    def __init__(self, copies, place, own, view, whole):
        self.copies, self.place, self.own, self.view = copies, place, own, view
        self.arrived = copies.reserve(place["z_count"])
        self.sent = copies.reserve_send(whole)

    def start(self):
        place = self.place
        for step in reversed(place["steps"]):
            self.copies.start(
                self.own,
                functools.partial(self.view, place["dp"]),
                {"dp": place["slots"][step]},
                self.sent,
                self.arrived + place["z"],
            )

    def forward(self, step):
        pass

    def settle(self, step):
        source, slot = self.place["order"][step], self.place["slots"][step]
        self.copies.wait(functools.partial(self.view, slot), self.arrived + source)


class Chain:
    def __init__(self, copies, place, own, view):
        self.copies, self.place, self.own, self.view = copies, place, own, view
        self.arrived = copies.reserve(place["z_count"])

    def start(self):
        place = self.place
        block = functools.partial(self.view, place["dp"])
        for way in (1, -1):
            onward = place["z"] + way
            when = place["above"] if way > 0 else place["below"]
            self.copies.start(
                self.own,
                block,
                {"dp": 2 * onward + place["side"]},
                self.copies.reserve_send(block, when),
                self.arrived + place["z"],
                when,
            )

    def passes(self, step):
        place, source = self.place, self.place["order"][step]
        rising = (source < place["z"]) & place["above"]
        sinking = (source > place["z"]) & place["below"]
        return rising, sinking

    def block(self, step):
        return functools.partial(self.view, self.place["slots"][step])

    def forward(self, step):
        place = self.place
        source, block = place["order"][step], self.block(step)
        rising, sinking = self.passes(step)
        sent = self.copies.reserve_send(block, rising | sinking)

        def move():
            self.copies.wait(block, self.arrived + source)
            for way in (1, -1):
                onward = place["z"] + way
                self.copies.start(
                    block,
                    block,
                    {"dp": 2 * onward + place["side"]},
                    sent,
                    self.arrived + source,
                    rising if way > 0 else sinking,
                )

        guarded(rising | sinking, move)

    def settle(self, step):
        source, block = self.place["order"][step], self.block(step)
        rising, sinking = self.passes(step)
        guarded(
            jnp.logical_not(rising | sinking),
            lambda: self.copies.wait(block, self.arrived + source),
        )


class PlaneSpread:
    def __init__(self, copies, place, view, span, rows, halves, sent):
        self.copies, self.place, self.view, self.rows = copies, place, view, rows
        self.span, self.halves, self.sent = span, halves, sent
        self.early_x, self.early_y, self.rest = (copies.reserve() for _ in range(3))

    def start(self, owner, begin, count, towards, recv_at):
        block = functools.partial(self.view, self.place[owner], begin, count)
        self.copies.start(block, block, {"sp": self.place[towards]}, self.sent, recv_at)

    def send(self):
        rows, half = self.rows, self.rows // 2
        if self.halves:
            self.start("me", 0, half, "x", self.early_x)
            self.start("me", half, half, "y", self.early_y)
            self.start("me", half, half, "x", self.rest)
            self.start("me", 0, half, "y", self.rest)
        else:
            self.start("me", 0, rows, "x", self.early_x)
            self.start("me", 0, rows, "y", self.early_y)

    def relay(self):
        half = self.rows // 2
        early = half if self.halves else self.rows
        self.copies.wait(functools.partial(self.view, self.place["x"], 0, early), self.early_x)
        self.start("x", 0, half, "y", self.rest)
        begin = half if self.halves else 0
        self.copies.wait(functools.partial(self.view, self.place["y"], begin, early), self.early_y)
        self.start("y", half, half, "x", self.rest)

    def finish(self):
        self.copies.wait(functools.partial(self.span, 4 if self.halves else 2), self.rest)


class Gather:
    def __init__(self, copies, place, buffer, groups):
        self.copies, self.place, self.buffer = copies, place, buffer
        self.crossed = [copies.reserve() for _ in range(groups)]
        self.cross_sent = copies.reserve_send(lambda: buffer.at[pl.ds(0, place["z_count"])])

    def cross(self, step, source, target):
        self.copies.start(
            source,
            target,
            {"dp": self.place["core"]},
            self.cross_sent,
            self.crossed[step % len(self.crossed)],
        )

    def keep(self):
        self.cross(0, self.own_whole, lambda: self.buffer.at[self.place["dp"]])

    def finish(self):
        self.copies.wait(lambda: self.buffer.at[pl.ds(0, self.place["z_count"])], self.crossed[0])

    def finish_step(self, step):
        self.copies.wait(lambda: self.buffer.at[0], self.crossed[step])


class WeightGather(Gather):
    def __init__(self, copies, place, source, buffer, tail=0, chunks=1, chained=False, halves=True):
        super().__init__(copies, place, buffer, place["z_count"] if chained else 1)
        self.own_whole = (lambda: source) if chained else (lambda: buffer.at[place["dp"]])
        self.rows = (source.shape[0] - tail) // place["sp_count"]
        self.halves = halves
        self.planes = {}
        self.plane_sent = copies.reserve_send(
            lambda: buffer.at[pl.ds(0, len(place["steps"])), pl.ds(0, 3 * self.rows), :]
        )
        start = pl.multiple_of(place["me"] * self.rows, SUBLANES)
        own = lambda: source.at[pl.ds(start, self.rows), :]
        view = lambda slot: self.piece(slot, place["me"], 0, self.rows)
        if chained:
            self.chain = Chain(copies, place, own, view)
        else:
            whole = lambda: source.at[pl.ds(0, self.rows * len(place["steps"])), :]
            self.chain = Direct(copies, place, lambda: view(place["dp"]), view, whole)
        if tail:
            part = tail // chunks
            self.tails = []
            for at in range(source.shape[0] - tail, source.shape[0], part):
                rest = pl.ds(at, part)
                view = lambda slot, rest=rest: buffer.at[slot, rest, :]
                own = lambda rest=rest: source.at[rest, :]
                self.tails.append(Chain(copies, place, own, view))

    def piece(self, slot, owner, begin, count):
        start = pl.multiple_of(owner * self.rows + begin, SUBLANES)
        return self.buffer.at[slot, pl.ds(start, count), :]

    def span(self, halves):
        return self.buffer.at[0, pl.ds(0, halves * (self.rows // 2)), :]

    def cross_piece(self, step, owner):
        slot = self.place["slots"][step]
        block = lambda: self.piece(slot, self.place[owner], 0, self.rows)
        self.cross(step, block, block)

    def spread(self, step):
        self.chain.settle(step)
        view = functools.partial(self.piece, self.place["slots"][step])
        plane = PlaneSpread(
            self.copies, self.place, view, self.span, self.rows, self.halves, self.plane_sent
        )
        plane.send()
        self.planes[step] = plane
        self.cross_piece(step, "me")

    def relay(self, step):
        self.planes[step].relay()
        if not self.halves:
            self.cross_piece(step, "x")
            self.cross_piece(step, "y")

    def close(self, step):
        self.planes[step].finish()
        if self.halves:
            self.cross_piece(step, "x")
            self.cross_piece(step, "y")
        self.cross_piece(step, "far")

    def start_tail(self, chunk):
        self.tails[chunk].start()

    def forward_tail(self, chunk, step):
        self.tails[chunk].forward(step)

    def settle_tail(self, chunk, step):
        tail = self.tails[chunk]
        tail.settle(step)
        self.cross(step, tail.block(step), tail.block(step))


class ColumnGather(Gather):
    def __init__(self, copies, place, source, buffer):
        super().__init__(copies, place, buffer, 1)
        width = buffer.shape[2]
        start = pl.multiple_of(place["me"] * width, LANES)
        self.own_whole = lambda: source.at[:, pl.ds(start, width)]
        self.view = lambda slot: buffer.at[slot]
        self.chain = Chain(copies, place, self.own_whole, self.view)

    def settle(self, step):
        self.chain.settle(step)
        slot = self.place["slots"][step]
        block = lambda: self.view(slot)
        self.cross(step, block, block)


def nearest_first(z, z_count, step):
    short = jnp.minimum(z, z_count - 1 - z)
    long_way = jnp.where(2 * z < z_count - 1, 1, -1)
    turn = (step + 1) // 2
    both = z - long_way * turn if step % 2 else z + long_way * turn
    return jnp.where(step <= 2 * short, both, z + long_way * (step - short))


def rotary_picks(rows, offset, skip):
    width = skip + 2 * ROPE
    row = lax.broadcasted_iota(jnp.int32, (rows, width), 0)
    col = lax.broadcasted_iota(jnp.int32, (rows, width), 1)
    half = ROPE // 2
    minus = (col >= skip + ROPE) & (col < skip + ROPE + half)
    origin = jnp.where(
        col < skip + ROPE, col, jnp.where(minus, col - half, col - ROPE - half)
    )
    sign = jnp.where(minus, -1.0, 1.0)
    return jnp.where(row == origin + offset, sign, 0.0).astype(jnp.bfloat16)


def turned(values, table):
    product = values * table
    return product + pltpu.roll(product, ROPE, axis=1)


def dot(left, right):
    return jnp.dot(left, right, preferred_element_type=jnp.float32)


def kernel(
    sp_count, dp_count,
    tokens_in, w_qdown, w_kvdown, rotary_in, q_gain_in, kv_gain_in, w_qup, w_kvup, w_out,
    out_gain_in, table_in,
    out,
    tokens, w_rotary, q_gain, kv_gain, out_gain, table,
    qd_all, kvd_all, qu_all, kvu_all, wo_all, q_lat, kv_lat, rot_all,
    q_heads, k_heads, v_heads, qu_laid, attended, merged, proj,
    send_sems, recv_sems, back_send, back_recv, local_sems,
):
    scope = jax.named_scope
    me = lax.axis_index("sp")
    dp = lax.axis_index("dp")
    z_count = dp_count // 2
    side = lax.rem(dp, 2)
    z = dp // 2
    steps = range(1, z_count)
    order = {step: nearest_first(z, z_count, step) for step in steps}
    place = {
        "me": me,
        "dp": dp,
        "z": z,
        "side": side,
        "above": z < z_count - 1,
        "below": z > 0,
        "order": order,
        "slots": {step: 2 * order[step] + side for step in steps},
        "sp_count": sp_count,
        "dp_count": dp_count,
        "z_count": z_count,
        "steps": steps,
        "x": me + 1 - 2 * lax.rem(me, 2),
        "y": lax.rem(me + 2, sp_count),
        "far": sp_count - 1 - me,
        "core": dp + 1 - 2 * side,
    }
    count = tokens.shape[0]
    heads = q_heads.shape[0]
    rank = kvd_all.shape[2]

    barrier = pltpu.get_barrier_semaphore()

    def greet(peer):
        pl.semaphore_signal(barrier, inc=1, device_id=peer, device_id_type=MESH)

    for step in range(1, sp_count):
        greet({"sp": lax.rem(me + step, sp_count)})
    greet({"dp": place["core"]})
    for step in steps:
        greet({"dp": lax.rem(dp + 2 * step, dp_count)})

    copies = Copies(send_sems, recv_sems)
    kvd = WeightGather(copies, place, w_kvdown, kvd_all)
    qd = WeightGather(copies, place, w_qdown, qd_all)
    kvu = ColumnGather(copies, place, w_kvup, kvu_all)
    qu = ColumnGather(copies, place, w_qup, qu_all)
    wo = WeightGather(copies, place, w_out, wo_all, w_out.shape[0] * 7 // 16, chunks=CHUNKS, chained=True)
    places = [
        (w_kvdown, kvd_all.at[dp]),
        (rotary_in, w_rotary),
        (tokens_in, tokens),
        (table_in, table),
        (w_qdown, qd_all.at[dp]),
        (kv_gain_in, kv_gain),
        (q_gain_in, q_gain),
        (out_gain_in, out_gain),
        (qu.own_whole(), qu_all.at[dp]),
        (kvu.own_whole(), kvu_all.at[dp]),
        (w_out, wo_all.at[dp]),
    ]
    loads = [
        pltpu.make_async_copy(source, target, local_sems.at[at])
        for at, (source, target) in enumerate(places)
    ]
    for load in loads:
        load.start()

    with scope("barrier"):
        pl.semaphore_wait(barrier, sp_count + len(steps))

    loads[0].wait()
    kvd.chain.start()
    kvd.keep()
    for load in loads[1:8]:
        load.wait()
    for gather in (qd, kvu, qu, wo):
        gather.keep()

    with scope("keyrot"):
        own_table = table[pl.ds(pl.multiple_of(me * count, SUBLANES), count), :]
        picks = rotary_picks(ROPE, 0, 0)
        rotary = lax.dot_general(
            picks, w_rotary[...], (((0,), (0,)), ((), ())), preferred_element_type=jnp.float32
        ).astype(jnp.bfloat16)
        key_rot = lax.dot_general(
            tokens[...], rotary, (((1,), (1,)), ((), ())), preferred_element_type=jnp.float32
        )
        key_rot = turned(key_rot, own_table)
        lane = lax.broadcasted_iota(jnp.int32, key_rot.shape, 1)
        rot_all[me] = jnp.where(lane < ROPE, key_rot, 0.0).astype(jnp.bfloat16)

    last = steps[-1]

    def block_view(buffer, owner, begin, rows):
        return buffer.at[owner, pl.ds(begin, rows), :]

    def latent_plane(buffer):
        sent = copies.reserve_send(lambda: buffer.at[pl.ds(0, 3)])
        span = lambda halves: buffer.at[pl.ds(0, halves // 2)]
        view = functools.partial(block_view, buffer)
        return PlaneSpread(copies, place, view, span, count, True, sent)

    rot_plane = latent_plane(rot_all)
    kv_plane = latent_plane(kv_lat)
    q_plane = latent_plane(q_lat)

    def make_kv_latent():
        down = kvd_all[...].reshape(-1, rank)
        kv_lat[me] = norm_rows(dot(tokens[...], down), kv_gain[...]).astype(jnp.bfloat16)

    def make_q_latent():
        down = qd_all[...].reshape(-1, qd_all.shape[2])
        q_lat[me] = norm_rows(dot(tokens[...], down), q_gain[...]).astype(jnp.bfloat16)

    def lay_queries():
        laid = qu_all[...].reshape(-1, qu_all.shape[2])
        for head in range(heads):
            picks = rotary_picks(laid.shape[1], head * (NOPE + ROPE), NOPE)
            qu_laid[:, head * head_width : (head + 1) * head_width] = dot(laid, picks).astype(
                jnp.bfloat16
            )

    head_width = NOPE + 2 * ROPE

    def do(name, action, *args):
        with scope(name + "".join(str(a) for a in args)):
            action(*args)

    def make_keys(block, _):
        rows = pl.ds(pl.multiple_of(block * count, SUBLANES), count)
        latent = kv_lat[block]
        full = dot(latent, kvu_all[...].reshape(rank, -1)).astype(jnp.bfloat16)
        for head in range(heads):
            at = head * (NOPE + VDIM)
            k_heads[head, rows, :NOPE] = full[:, at : at + NOPE]
            k_heads[head, rows, NOPE:] = rot_all[block]
            v_heads[head, rows, :] = full[:, at + NOPE : at + NOPE + VDIM]
        return 0

    def make_all_keys():
        lax.fori_loop(0, sp_count, make_keys, 0)

    def make_block(block, _):
        rows = pl.ds(pl.multiple_of(block * count, SUBLANES), count)
        full = dot(q_lat[block], qu_laid[...])
        turns = table[rows, :]
        for head in range(heads):
            at = head * head_width
            q_heads[head, rows, :NOPE] = full[:, at : at + NOPE].astype(jnp.bfloat16)
            part = full[:, at + NOPE : at + head_width]
            q_heads[head, rows, NOPE:] = turned(part, turns).astype(jnp.bfloat16)
        return 0

    def make_all_queries():
        lax.fori_loop(0, sp_count, make_block, 0)

    factor = (NOPE + ROPE) ** (-0.5) * math.log2(math.e)
    contract = (((1,), (1,)), ((), ()))
    width = heads * VDIM

    def head_lanes(owner, head):
        return pl.ds(pl.multiple_of(owner * width + head * VDIM, LANES), VDIM)

    def merged_lanes(source, head):
        return pl.ds(pl.multiple_of(head * (sp_count * VDIM) + source * VDIM, LANES), VDIM)

    def back(block, head, source):
        return pltpu.make_async_remote_copy(
            src_ref=attended.at[block, :, head_lanes(0, head)],
            dst_ref=merged.at[:, merged_lanes(source, head)],
            send_sem=back_send,
            recv_sem=back_recv.at[head],
            device_id={"sp": block},
            device_id_type=MESH,
        )

    def one_head(head, _):
        for block in reversed(range(sp_count)):
            begin = block * count
            query = q_heads[head, begin : begin + count, :]
            near = lax.dot_general(
                query, k_heads[head, begin : begin + count, :], contract,
                preferred_element_type=jnp.float32,
            )
            row = lax.broadcasted_iota(jnp.int32, near.shape, 0)
            col = lax.broadcasted_iota(jnp.int32, near.shape, 1)
            near = jnp.where(col <= row, near, -jnp.inf)
            top = jnp.max(near, axis=-1, keepdims=True)
            if block:
                far = lax.dot_general(
                    query, k_heads[head, :begin, :], contract, preferred_element_type=jnp.float32
                )
                top = jnp.maximum(top, jnp.max(far, axis=-1, keepdims=True))
            near = jnp.exp2((near - top) * factor)
            total = jnp.sum(near, axis=-1, keepdims=True)
            if block:
                far = jnp.exp2((far - top) * factor)
                total = total + jnp.sum(far, axis=-1, keepdims=True)
            share = 1.0 / total
            result = dot((near * share).astype(jnp.bfloat16), v_heads[head, begin : begin + count, :])
            if block:
                result = result + dot((far * share).astype(jnp.bfloat16), v_heads[head, :begin, :])
            attended[block, :, head_lanes(0, head)] = result.astype(jnp.bfloat16)
        for block in range(sp_count):

            @pl.when(me != block)
            def _():
                back(block, head, me).start()

        merged[:, merged_lanes(me, head)] = attended[me, :, head_lanes(0, head)]
        return 0

    def attend_head(head):
        lax.fori_loop(head, head + 1, one_head, 0)

    others = attended.at[pl.ds(0, sp_count - 1)]
    out_width = wo_all.shape[2]

    def wait_back(begin, finish):
        for head in range(begin, finish):
            part = attended.at[pl.ds(0, sp_count - 1), :, head_lanes(0, head)]
            pltpu.make_async_copy(part, part, back_recv.at[head]).wait()

    def project(step, begin, finish):
        squares = jnp.zeros((count, 1), jnp.float32)
        for core in range(2):
            piece = 2 * (order[step] if step else z) + core
            lanes = pl.ds(pl.multiple_of(piece * out_width, LANES), out_width)
            rows = [
                wo_all[piece, pl.ds(source * width + head * VDIM, VDIM), :]
                for head in range(begin, finish)
                for source in range(sp_count)
            ]
            whole = sp_count * VDIM
            value = dot(merged[:, begin * whole : finish * whole], jnp.concatenate(rows, axis=0))
            if begin:
                value = value + proj[:, lanes]
            proj[:, lanes] = value
            if finish == heads:
                squares = squares + jnp.sum(value * value, axis=-1, keepdims=True)
        return squares

    rot_plane.send()
    do("kd_s", kvd.spread, 1)
    do("kd_s", kvd.spread, 2)
    do("rot_r", rot_plane.relay)
    qd.chain.start()
    do("kd_s", kvd.spread, 3)
    do("kd_r", kvd.relay, 1)
    kvu.chain.start()
    qu.chain.start()
    wo.chain.start()
    do("kd_r", kvd.relay, 2)
    do("kd_r", kvd.relay, 3)
    do("qd_s", qd.spread, 1)
    do("kd_c", kvd.close, 1)
    do("qd_s", qd.spread, 2)
    do("qd_s", qd.spread, 3)
    do("kd_c", kvd.close, 2)
    do("kd_c", kvd.close, 3)
    do("qd_r", qd.relay, 1)
    do("kvu_fw", kvu.chain.forward, 1)
    do("qu_fw", qu.chain.forward, 1)
    do("kvu_fw", kvu.chain.forward, 2)
    do("qu_fw", qu.chain.forward, 2)
    wo.start_tail(0)
    do("qd_r", qd.relay, 2)
    do("kd_f", kvd.finish)
    do("kv_lat", make_kv_latent)
    do("qd_r", qd.relay, 3)
    kv_plane.send()
    do("kvu_fw", kvu.chain.forward, 3)
    do("qu_fw", qu.chain.forward, 3)
    do("qd_c", qd.close, 1)
    do("qd_c", qd.close, 2)
    do("kv_r", kv_plane.relay)
    do("qd_c", qd.close, 3)
    do("qd_f", qd.finish)
    do("q_lat", make_q_latent)
    q_plane.send()
    do("wo_fw", wo.chain.forward, 1)
    do("wo_fw", wo.chain.forward, 2)
    do("q_r", q_plane.relay)
    do("wo_s", wo.spread, 1)
    do("wo_fw", wo.chain.forward, 3)
    do("t0_fw", wo.forward_tail, 0, 1)
    do("t0_fw", wo.forward_tail, 0, 2)
    wo.start_tail(1)
    do("qu_st", qu.settle, 1)
    do("kvu_st", kvu.settle, 1)
    do("qu_st", qu.settle, 2)
    do("kvu_st", kvu.settle, 2)
    do("qu_st", qu.settle, 3)
    do("kvu_st", kvu.settle, 3)
    loads[9].wait()
    do("kvu_f", kvu.finish)
    do("rot_f", rot_plane.finish)
    do("kv_f", kv_plane.finish)
    do("make_keys", make_all_keys)
    loads[8].wait()
    do("qu_f", qu.finish)
    do("qu_lay", lay_queries)
    do("wo_s", wo.spread, 2)
    do("q_f", q_plane.finish)
    do("make_q", make_all_queries)
    do("t0_fw", wo.forward_tail, 0, 3)
    do("wo_r", wo.relay, 1)
    do("attn", attend_head, 0)
    do("wo_s", wo.spread, 3)
    do("t1_fw", wo.forward_tail, 1, 1)
    do("t1_fw", wo.forward_tail, 1, 2)
    do("attn", attend_head, 1)
    do("wo_r", wo.relay, 2)
    do("attn", attend_head, 2)
    do("t1_fw", wo.forward_tail, 1, 3)
    do("wo_r", wo.relay, 3)
    do("attn", attend_head, 3)
    do("wo_c", wo.close, 1)
    do("t0_st", wo.settle_tail, 0, 1)
    do("t0_st", wo.settle_tail, 0, 2)
    do("t0_st", wo.settle_tail, 0, 3)
    do("t1_st", wo.settle_tail, 1, 1)
    do("wo_c", wo.close, 2)
    do("t1_st", wo.settle_tail, 1, 2)
    do("a2a", wait_back, 0, 3)
    squares = jnp.zeros((count, 1), jnp.float32)
    loads[10].wait()
    do("wo_f", wo.finish_step, 0)
    with scope("project00"):
        project(0, 0, 3)
    do("wo_f", wo.finish_step, 1)
    with scope("project10"):
        project(1, 0, 3)
    do("wo_f", wo.finish_step, 2)
    with scope("project20"):
        project(2, 0, 3)
    do("wo_c", wo.close, 3)
    do("a2a", wait_back, 3, 4)
    with scope("project03"):
        squares = squares + project(0, 3, 4)
    with scope("project13"):
        squares = squares + project(1, 3, 4)
    with scope("project23"):
        squares = squares + project(2, 3, 4)
    do("t1_st", wo.settle_tail, 1, 3)
    do("wo_f", wo.finish_step, 3)
    with scope("project30"):
        squares = squares + project(3, 0, 4)
    with scope("norm"):
        scale = lax.rsqrt(squares * (1.0 / out.shape[1]) + EPSILON)
        out[...] = (proj[...] * scale * out_gain[...]).astype(out.dtype)
    with scope("drain"):
        copies.drain()
        pltpu.make_async_copy(others, others, back_send).wait()


def kernel_body(mesh, tokens, w_qdown, w_kvdown, w_rotary, q_gain, kv_gain, w_qup, w_kvup, w_out, out_gain):
    sp_count, dp_count = mesh.shape["sp"], mesh.shape["dp"]
    heads = HEADS // sp_count
    count, depth = tokens.shape[1:]
    length = count * sp_count
    q_rank, kv_rank = w_qdown.shape[1], w_kvdown.shape[1]
    bf16 = jnp.bfloat16
    steps = dp_count // 2 - 1
    chains = 3 + CHUNKS
    sends = chains * (steps + 2) + 13
    receives = 3 * 3 * steps + 9 + (chains + 2) * (steps + 1) + 4 + steps + 1
    vmem, hbm = pl.BlockSpec(memory_space=pltpu.VMEM), pl.BlockSpec(memory_space=pl.ANY)
    sp_width = HEADS // sp_count
    mixed = pl.pallas_call(
        functools.partial(kernel, sp_count, dp_count),
        out_shape=pltpu.VMEM((count, w_out.shape[1] * dp_count), bf16),
        in_specs=[hbm] * 11,
        out_specs=vmem,
        scratch_shapes=[
            pltpu.VMEM((count, depth), bf16),
            pltpu.VMEM(w_rotary.shape[::-1], bf16),
            pltpu.VMEM((1, q_rank), jnp.float32),
            pltpu.VMEM((1, kv_rank), jnp.float32),
            pltpu.VMEM((1, out_gain.shape[0]), jnp.float32),
            pltpu.VMEM((length, 4 * (ROPE // 2)), jnp.float32),
            pltpu.VMEM((dp_count,) + w_qdown.shape, bf16),
            pltpu.VMEM((dp_count,) + w_kvdown.shape, bf16),
            pltpu.VMEM((dp_count, w_qup.shape[0], sp_width * (NOPE + ROPE)), bf16),
            pltpu.VMEM((dp_count, w_kvup.shape[0], sp_width * (NOPE + VDIM)), bf16),
            pltpu.VMEM((dp_count,) + w_out.shape, bf16),
            pltpu.VMEM((sp_count, count, q_rank), bf16),
            pltpu.VMEM((sp_count, count, kv_rank), bf16),
            pltpu.VMEM((sp_count, count, 2 * ROPE), bf16),
            pltpu.VMEM((heads, length, NOPE + 2 * ROPE), bf16),
            pltpu.VMEM((heads, length, NOPE + 2 * ROPE), bf16),
            pltpu.VMEM((heads, length, VDIM), bf16),
            pltpu.VMEM((q_rank, heads * (NOPE + 2 * ROPE)), bf16),
            pltpu.VMEM((sp_count, count, heads * VDIM), bf16),
            pltpu.VMEM((count, HEADS * VDIM), bf16),
            pltpu.VMEM((count, w_out.shape[1] * dp_count), jnp.float32),
            pltpu.SemaphoreType.DMA((sends,)),
            pltpu.SemaphoreType.DMA((receives,)),
            pltpu.SemaphoreType.DMA,
            pltpu.SemaphoreType.DMA((heads,)),
            pltpu.SemaphoreType.DMA((11,)),
        ],
        compiler_params=pltpu.CompilerParams(
            collective_id=0, has_side_effects=True, vmem_limit_bytes=60 * 1024 * 1024
        ),
        name="latent_attention",
    )(
        tokens[0], w_qdown, w_kvdown, w_rotary.T, q_gain[None], kv_gain[None], w_qup, w_kvup, w_out,
        out_gain[None], jnp.asarray(turn_table(length)),
    )
    return mixed[None]


def fits_kernel(mesh):
    return mesh.shape["sp"] == 2 * 2 and mesh.shape["dp"] % 2 == 0


def solution(mesh):
    in_specs = (
        P("dp", "sp", None),
        P("dp", None),
        P("dp", None),
        P(),
        P(),
        P(),
        P("dp", None),
        P("dp", None),
        P(None, "dp"),
        P(),
    )
    out_specs = P("dp", "sp", None)
    body = functools.partial(kernel_body, mesh) if fits_kernel(mesh) else plain_body
    return jax.shard_map(body, mesh=mesh, in_specs=in_specs, out_specs=out_specs, check_vma=False)
```
